256 devices in a mesh: grp: 2 (over y), sp: 32 (over z, core), tp: 4 (over x).
Axes of the slice: x: 4, y: 2, z: 16, core: 2. Of those that a mesh axis runs over, the one named last changes fastest.
The devices are a block of a 4x16x16 slice.
Arguments:
- queries: bfloat16 [16384, 1024], P(('grp', 'sp'), 'tp'), parts along dimension 0, may hold values from -7 to 10
- keys: bfloat16 [16384, 1024], P(('grp', 'sp'), 'tp'), parts along dimension 0, may hold values from -14 to 7
- values: bfloat16 [16384, 1024], P(('grp', 'sp'), 'tp'), parts along dimension 0, may hold values from -6 to 6
- resid: bfloat16 [16384, 2048], P(('grp', 'sp', 'tp')), parts along dimension 0, may hold values from -18 to 18
- out_weight: bfloat16 [1024, 2048], P('tp'), may hold values from -0.375 to 0.375
- gate_weight: bfloat16 [2048, 3072], P('sp', 'tp'), may hold values from -0.125 to 0.125
- value_weight: bfloat16 [2048, 3072], P('sp', 'tp'), may hold values from -0.125 to 0.125
- conv_gate: float32 [3, 3072], P(None, 'tp'), may hold values from -3 to 3
- conv_value: float32 [3, 3072], P(None, 'tp'), may hold values from -3 to 3
- norm_gain: float32 [2048], replicated, may hold values from 0.1 to 1.9
- down_weight: bfloat16 [3072, 2048], P('tp', 'sp'), may hold values from -0.109375 to 0.109375
Outputs:
- layer_out: bfloat16 [16384, 2048], P(('grp', 'sp', 'tp')), parts along dimension 0
The draws below stay inside these ranges and needn't reach their ends.
There are 2 independent parts, one for each index of `grp`. The reference program is written for one: setup_inputs(seed, part) draws one part's arguments, and reference() takes and returns one part's arrays. A program takes and returns all parts, laid end to end along the dimension named above; an argument that names none is the same for every part. Nothing has to cross between parts.
All inputs are finite; a program needn't handle non-finite values.
Results may differ from the reference program's by a relative error of at most 0.0058.
Values may be sent and summed in bfloat16 or wider, within the bound.
A program may use at most 128 MiB of HBM per device.

```python
import math
import jax
import jax.numpy as jnp
from jax import lax

D = 2048
HEAD_TOTAL = 16
HEAD = 64
FF = 3072
CONV = 3
TOK_DEV = 256
MIX = 1024
TOKEN_POSITIONS = 8192
KEY_BLOCK = 1024


def attention_pair(key):
    parallel_flows = jax.random.split(jax.random.fold_in(key, 11), 7)
    shape = (TOKEN_POSITIONS, HEAD_TOTAL, HEAD)
    query_noise = jnp.clip(jax.random.normal(parallel_flows[0], shape, jnp.float32), -4.5, 4.5)
    key_noise = jnp.clip(jax.random.normal(parallel_flows[1], shape, jnp.float32), -4.5, 4.5)
    fast_share = 0.5
    query_noise = query_noise * 1.4
    key_noise = key_noise * 1.4
    fast = jax.random.uniform(parallel_flows[2], (HEAD_TOTAL,), jnp.float32) < fast_share
    slow_level = -math.log(TOKEN_POSITIONS) - 2.0
    level = jnp.where(fast, -4.5, slow_level)
    block_shift = jax.random.uniform(parallel_flows[3], (TOKEN_POSITIONS // TOK_DEV, HEAD_TOTAL), jnp.float32, -0.7, 0.7)
    start_displacement = level[None, :] + jnp.repeat(block_shift, TOK_DEV, axis=0)
    surge_location = jax.random.randint(parallel_flows[4], (3, HEAD_TOTAL), 0, TOKEN_POSITIONS)
    surge_level = jax.random.uniform(parallel_flows[5], (3, HEAD_TOTAL), jnp.float32, -1.4, 0.0)
    token_position = jnp.arange(TOKEN_POSITIONS, dtype=jnp.int32)
    match_count = token_position[:, None, None] == surge_location[None, :, :]
    surge_value = jnp.max(jnp.where(match_count, surge_level[None, :, :], -100.0), axis=1)
    start_displacement = jnp.where(jnp.any(match_count, axis=1), surge_value, start_displacement)
    query_lead = 8.0 + 0.3 * jnp.clip(jax.random.normal(parallel_flows[6], (TOKEN_POSITIONS, HEAD_TOTAL), jnp.float32), -3.0, 3.0)
    query_full = query_noise.at[:, :, 0].set(query_lead)
    key_full = key_noise.at[:, :, 0].set(start_displacement)
    return (query_full.reshape(TOKEN_POSITIONS, HEAD_TOTAL * HEAD), key_full.reshape(TOKEN_POSITIONS, HEAD_TOTAL * HEAD))


def draw_queries(key, part):
    return attention_pair(key)[0].astype(jnp.bfloat16)


def draw_keys(key, part):
    return attention_pair(key)[1].astype(jnp.bfloat16)


def draw_resid(key, part):
    parallel_flows = jax.random.split(jax.random.fold_in(key, 23), 3)
    base = jnp.clip(jax.random.normal(parallel_flows[0], (TOKEN_POSITIONS, D), jnp.float32), -3.0, 3.0)
    reach = 0.6
    column_scale = jnp.exp(jax.random.uniform(parallel_flows[1], (D,), jnp.float32, -reach, reach))
    row_scale = jnp.exp(jax.random.uniform(parallel_flows[2], (TOKEN_POSITIONS,), jnp.float32, -reach, reach))
    return (base * row_scale[:, None] * column_scale[None, :]).astype(jnp.bfloat16)


def block_levels(rng, dims, cuts, low, top_value):
    gain, own = 1.0, jax.random.fold_in(rng, 6)
    for position, parts in cuts:
        steps = jnp.exp(jax.random.uniform(jax.random.fold_in(own, position), (parts,), jnp.float32, low / len(cuts), top_value / len(cuts)))
        gain = gain * jnp.repeat(steps, dims[position] // parts).reshape([-1 if axis == position else 1 for axis in range(len(dims))])
    return gain


def normal_values(key, dims, deviation, most, cuts=(), held_as=jnp.bfloat16):
    array = jax.random.normal(key, dims, jnp.float32) * deviation
    if len(cuts) > 0:
        array = block_levels(key, dims, cuts, -0.22, 0.18) * array
    return jnp.clip(array, min=-most, max=most).astype(held_as)


def setup_inputs(seed: int = 0, part: int = 0) -> dict:
    key_of = jax.random.split(jax.random.key(seed), 12)
    own_keys = jax.random.split(jax.random.fold_in(key_of[11], part), 12)
    queries = draw_queries(jax.random.fold_in(jax.random.fold_in(key_of[11], part), 71), part)
    keys = draw_keys(jax.random.fold_in(jax.random.fold_in(key_of[11], part), 71), part)
    values = normal_values(own_keys[2], (TOKEN_POSITIONS, MIX), 1.0, 6.0, ((0, 32), (1, 4)))
    resid = draw_resid(jax.random.fold_in(jax.random.fold_in(key_of[11], part), 71), part)
    out_weight = normal_values(key_of[4], (MIX, D), (MIX // 4) ** -0.5, 0.375, ((0, 4),))
    gate_weight = normal_values(key_of[5], (D, FF), D ** -0.5, 0.125, ((0, 32), (1, 4)))
    value_weight = normal_values(key_of[6], (D, FF), D ** -0.5, 0.125, ((0, 32), (1, 4)))
    conv_gate = normal_values(key_of[7], (CONV, FF), 0.5, 3.0, ((1, 4),), jnp.float32)
    conv_value = normal_values(key_of[8], (CONV, FF), 0.5, 3.0, ((1, 4),), jnp.float32)
    norm_gain = jnp.clip(1.0 + 0.18 * jax.random.normal(key_of[9], (D,), jnp.float32), 0.1, 1.9)
    down_weight = normal_values(key_of[10], (FF, D), FF ** -0.5, 0.109375, ((0, 4), (1, 32)))
    return dict(queries=queries, keys=keys, values=values, resid=resid, out_weight=out_weight, gate_weight=gate_weight, value_weight=value_weight, conv_gate=conv_gate, conv_value=conv_value, norm_gain=norm_gain, down_weight=down_weight)


epsilon = 1e-06

def block_terms(query_rows, key_rows, value_rows, query_place, key_place):
    scores = jnp.einsum('qhe,khe->hqk', query_rows.astype(jnp.float32), key_rows.astype(jnp.float32)) * HEAD ** (-0.5)
    causal = (key_place[None, :] < query_place[:, None])[None]
    stay_log = jnp.where(causal, jax.nn.log_sigmoid(-scores), 0.0)
    suffix = lax.cumsum(stay_log, axis=2, reverse=True) - stay_log
    local_weight = jnp.where(causal, jnp.exp(jax.nn.log_sigmoid(scores) + suffix), 0.0).astype(jnp.bfloat16)
    part = jnp.einsum('hqk,khe->hqe', local_weight.astype(jnp.float32), value_rows.astype(jnp.float32))
    return (lax.optimization_barrier(jnp.sum(stay_log, axis=2)), part)

def attend(queries, keys, values):
    count = TOKEN_POSITIONS // KEY_BLOCK
    query_all = queries.reshape(count, KEY_BLOCK, HEAD_TOTAL, HEAD)
    key_all = keys.reshape(count, KEY_BLOCK, HEAD_TOTAL, HEAD)
    value_all = values.reshape(count, KEY_BLOCK, HEAD_TOTAL, HEAD)
    block_ids = jnp.arange(count, dtype=jnp.int32)

    def per_query(inputs):
        query_rows, query_id = inputs
        query_place = query_id * KEY_BLOCK + jnp.arange(KEY_BLOCK, dtype=jnp.int32)

        def add_block(carry, pieces):
            key_rows, value_rows, key_id = pieces
            key_place = key_id * KEY_BLOCK + jnp.arange(KEY_BLOCK, dtype=jnp.int32)
            total, part = block_terms(query_rows, key_rows, value_rows, query_place, key_place)
            return (carry * jnp.exp(total)[:, :, None] + part, None)
        start_carry = jnp.zeros((HEAD_TOTAL, KEY_BLOCK, HEAD), jnp.float32)
        result, _ = lax.scan(add_block, start_carry, (key_all, value_all, block_ids))
        return result
    attended = lax.map(per_query, (query_all, block_ids))
    return jnp.transpose(attended, (0, 2, 1, 3)).reshape(TOKEN_POSITIONS, HEAD_TOTAL * HEAD).astype(jnp.bfloat16)

def normalize(state, norm_gain):
    values = state.astype(jnp.float32)
    scaled = values * lax.rsqrt(lax.optimization_barrier(jnp.mean(values * values, axis=-1, keepdims=True)) + epsilon)
    return (scaled * norm_gain.astype(jnp.float32)).astype(jnp.bfloat16)

def causal_conv(rows, taps):
    length = rows.shape[0]
    padded = jnp.pad(rows.astype(jnp.float32), ((taps.shape[0] - 1, 0), (0, 0)))
    total = jnp.zeros(rows.shape, jnp.float32)
    for start_displacement in range(taps.shape[0]):
        total = total + taps[start_displacement].astype(jnp.float32) * padded[start_displacement:start_displacement + length]
    return total

def reference(queries, keys, values, resid, out_weight, gate_weight, value_weight, conv_gate, conv_value, norm_gain, down_weight):
    mixed = attend(queries, keys, values)
    projected = jnp.dot(mixed, out_weight, preferred_element_type=jnp.float32)
    state = (resid.astype(jnp.float32) + projected).astype(jnp.bfloat16)
    normed = normalize(state, norm_gain)
    gate_pre = jnp.dot(normed, gate_weight, preferred_element_type=jnp.float32).astype(jnp.bfloat16)
    value_pre = jnp.dot(normed, value_weight, preferred_element_type=jnp.float32).astype(jnp.bfloat16)
    conv_gate_out = causal_conv(gate_pre, conv_gate)
    conv_value_out = causal_conv(value_pre, conv_value)
    gated = (jax.nn.silu(conv_gate_out) * conv_value_out).astype(jnp.bfloat16)
    ffn = jnp.dot(gated, down_weight, preferred_element_type=jnp.float32)
    return (state.astype(jnp.float32) + ffn).astype(jnp.bfloat16)
```

```python
import functools
import math

import jax
import jax.numpy as jnp
from jax import lax
from jax.experimental import pallas as pl
from jax.experimental.pallas import tpu as pltpu
from jax.sharding import PartitionSpec as P

HEAD = 64
LANES = 128
EPS = 1e-06
GROUPS = 4
HALO = 16
MESH = pl.DeviceIdType.MESH
F32 = jnp.float32
BF16 = jnp.bfloat16
LOG2E = math.log2(math.e)


def kernel(
    dims,
    q_ref, k_ref, v_ref, resid_ref, wo_ref, gw_ref, vw_ref, cg_ref, cv_ref, gain_ref, dw_ref,
    out_ref,
    pack, s1, s2, kv, qx, tri, acc, later, mo, m2, wo, wf, dpart, state, ext, gated, rsb, pf, rsr,
    s1_s, s1_r, s2_s, s2_r, s3_s, s3_r, sp_s, sp_r, cw_s, cw_r, cc_s, cc_r, wp_s, wp_r,
    wo_l, wo_s, wo_r, wop_s, wop_r, m2_s, m2_r, nx_s, nx_r, ha_s, ha_r, rs_s, rs_r, dp_s, dp_r,
):
    nx, nz, heads, tok, piece, width, ff, slab = dims
    half = piece // 2
    down_rows = ff // 2
    blocks = down_rows // slab
    strips = nz // GROUPS
    rows_group = strips * piece
    sp = lax.axis_index("sp")
    x = lax.axis_index("tp")
    z = lax.div(sp, 2)
    c = lax.rem(sp, 2)
    partner = z * 2 + 1 - c
    low = lambda rows: lax.broadcasted_iota(jnp.int32, (rows, LANES), 1) < HEAD
    swap = lambda a: pltpu.roll(a, HEAD, 1)

    def xat(d):
        return lax.rem(x + d + nx, nx)

    def zat(d):
        return lax.rem(z + d + nz, nz)

    def remote(src, dst, send, recv, **where):
        return pltpu.make_async_remote_copy(
            src_ref=src, dst_ref=dst, send_sem=send, recv_sem=recv, device_id=where,
            device_id_type=MESH,
        )

    def slab_rows(zz, cc):
        return pl.ds(pl.multiple_of((zz * 2 + cc) * slab, slab), slab)

    for xp in range(nx):
        at = xp * piece
        for p in range(heads // 2):
            cols = slice(p * LANES, (p + 1) * LANES)
            kk = k_ref[at : at + piece, cols].astype(F32)
            vv = v_ref[at : at + piece, cols].astype(F32)
            qq = q_ref[at : at + piece, cols].astype(F32)
            qr = swap(qq)
            keep = low(piece)
            pack[xp, 2 * p, 0:piece] = jnp.where(keep, kk, swap(vv)).astype(BF16)
            pack[xp, 2 * p + 1, 0:piece] = jnp.where(keep, swap(kk), vv).astype(BF16)
            keep = low(half)
            pack[xp, 2 * p, piece:] = jnp.where(keep, qq[:half], qr[half:]).astype(BF16)
            pack[xp, 2 * p + 1, piece:] = jnp.where(keep, qr[:half], qq[half:]).astype(BF16)
    s1[x] = pack[x]
    wf[slab_rows(z, c), 0:ff] = gw_ref[...]
    wf[slab_rows(z, c), ff : 2 * ff] = vw_ref[...]

    own_wo = pltpu.make_async_copy(wo_ref, wo.at[x], wo_l)
    own_wo.start()

    barrier = pltpu.get_barrier_semaphore()
    last_x = x == nx - 1
    before = lax.rem(sp + 2 * nz - 1, 2 * nz)
    after = lax.rem(sp + 1, 2 * nz)

    def greet(**where):
        pl.semaphore_signal(barrier, inc=1, device_id=where, device_id_type=MESH)

    for d in range(1, nx):
        greet(tp=xat(d))
    for d in range(1, nz):
        greet(sp=zat(d) * 2 + c)
    greet(sp=partner)
    greet(sp=before, tp=nx - 1)

    @pl.when(last_x)
    def _():
        for xp in range(nx):
            greet(sp=after, tp=xp)

    pl.semaphore_wait(barrier, nx - 1 + nz - 1 + 2 + jnp.where(last_x, nx, 0))

    ends = []
    for d in range(1, nx):
        copy = remote(pack.at[xat(d)], s1.at[x], s1_s.at[d - 1], s1_r.at[d - 1], tp=xat(d))
        copy.start()
        ends.append(copy)
    down_part = remote(
        dw_ref.at[pl.ds(pl.multiple_of((1 - c) * down_rows, slab), down_rows)], dpart, dp_s, dp_r,
        sp=partner,
    )
    down_part.start()
    ends.append(down_part)
    share = wo_ref.shape[0] // 2
    own_half = pl.ds(pl.multiple_of(c * share, share), share)
    for d in range(1, nx):
        copy = remote(
            wo_ref.at[own_half], wo.at[x, own_half], wo_s.at[d - 1], wo_r.at[d - 1], tp=xat(d)
        )
        copy.start()
        ends.append(copy)

    down_part.wait_recv()
    mine = dw_ref[pl.ds(pl.multiple_of(c * down_rows, slab), down_rows), :].astype(F32)
    other = dpart[...].astype(F32)
    first = c == 0
    row = lax.broadcasted_iota(jnp.int32, (HEAD, LANES), 0)
    col = lax.broadcasted_iota(jnp.int32, (HEAD, LANES), 1)
    place_low = (row == col).astype(BF16)
    place_high = (row + HEAD == col).astype(BF16)
    both = jnp.dot(
        jnp.where(first, mine, other).astype(BF16), place_low, preferred_element_type=F32
    ) + jnp.dot(jnp.where(first, other, mine).astype(BF16), place_high, preferred_element_type=F32)
    both = both.astype(BF16)
    for j in range(blocks):
        wf[slab_rows(z, c), 2 * ff + j * LANES : 2 * ff + (j + 1) * LANES] = both[
            j * slab : (j + 1) * slab
        ]
    up_hops = nz // 2
    down_hops = nz - 1 - up_hops

    def pass_slab(origin, step):
        rows = wf.at[slab_rows(origin, c)]
        return rows

    def send_up(step):
        rows = pass_slab(zat(-step), step)
        copy = remote(rows, rows, cw_s.at[step], cw_r.at[step], sp=zat(1) * 2 + c)
        copy.start()
        ends.append(copy)

    def send_down(step):
        rows = pass_slab(zat(step), step)
        copy = remote(rows, rows, cc_s.at[step], cc_r.at[step], sp=zat(-1) * 2 + c)
        copy.start()
        ends.append(copy)

    def send_across(origin, index):
        rows = pass_slab(origin, index)
        copy = remote(rows, rows, wp_s.at[index], wp_r.at[index], sp=partner)
        copy.start()
        ends.append(copy)

    send_up(0)
    send_down(0)
    send_across(z, 0)

    def serve(step):
        if step <= up_hops:
            rows = pass_slab(zat(-step), step)
            remote(rows, rows, cw_s.at[step - 1], cw_r.at[step - 1], sp=zat(1) * 2 + c).wait_recv()
            if step < up_hops:
                send_up(step)
            send_across(zat(-step), step)
        if step <= down_hops:
            rows = pass_slab(zat(step), step)
            remote(rows, rows, cc_s.at[step - 1], cc_r.at[step - 1], sp=zat(-1) * 2 + c).wait_recv()
            if step < down_hops:
                send_down(step)
            send_across(zat(step), nz - step)

    for d in range(1, nx):
        remote(
            pack.at[x], s1.at[xat(-d)], s1_s.at[d - 1], s1_r.at[d - 1], tp=xat(d)
        ).wait_recv()
    s2[z] = s1[lax.div(z, heads), lax.rem(z, heads)]
    order = sorted(range(1, nz), key=lambda d: (min(d, nz - d), d))
    for d in order:
        h = zat(d)
        copy = remote(
            s1.at[lax.div(h, heads), lax.rem(h, heads)], s2.at[z], s2_s.at[d - 1], s2_r.at[d - 1],
            sp=h * 2 + c,
        )
        copy.start()
        ends.append(copy)

    r = lax.broadcasted_iota(jnp.int32, (tok, tok), 0)
    s = lax.broadcasted_iota(jnp.int32, (tok, tok), 1)
    tri[...] = (r > s).astype(BF16)
    acc[...] = jnp.zeros_like(acc)
    later[...] = jnp.zeros_like(later)
    for d in [0] + order:
        zs = zat(-d)
        if d:
            remote(
                s2.at[z], s2.at[zs], s2_s.at[d - 1], s2_r.at[d - 1], sp=zat(d) * 2 + c
            ).wait_recv()
        kv[zs, c, x] = s2[zs, 0:piece]
        for e in range(1, nx):
            remote(
                s2.at[zs, 0:piece], kv.at[zs, c, x], s3_s.at[e - 1], s3_r.at[e - 1], tp=xat(e)
            ).start()
        packed = s2[zs, piece:].astype(F32)
        keep = low(half)
        at = pl.multiple_of(zs * piece, piece)
        qx[pl.ds(at, half)] = jnp.where(keep, packed, 0.0).astype(BF16)
        qx[pl.ds(pl.multiple_of(at + half, half), half)] = jnp.where(
            keep, swap(packed), 0.0
        ).astype(BF16)
    across = remote(
        s2.at[:, 0:piece], kv.at[:, c, x], sp_s.at[0], sp_r.at[0], sp=partner
    )
    across.start()
    ends.append(across)
    serve(1)
    for e in (1, nx - 1) + tuple(range(2, nx - 1)) if nx > 2 else (1,):
        source = xat(-e)
        got = kv.at[:, c, source]
        remote(
            s2.at[:, 0:piece], got, s3_s.at[e - 1], s3_r.at[e - 1], tp=xat(e)
        ).wait_recv()
        across = remote(got, got, sp_s.at[e], sp_r.at[e], sp=partner)
        across.start()
        ends.append(across)
    for e in range(nx):
        there = kv.at[:, 1 - c, xat(-e)]
        remote(there, there, sp_s.at[e], sp_r.at[e], sp=partner).wait_recv()
    serve(2)

    scale = LOG2E / math.sqrt(HEAD)

    def tile_step(j, g, masked):
        rows = slice(g * rows_group, (g + 1) * rows_group)
        tile = kv[lax.div(j, 2), lax.rem(j, 2)].reshape(tok, LANES)
        score = lax.dot_general(
            qx[rows], tile, (((1,), (1,)), ((), ())), preferred_element_type=F32
        ) * scale
        neg = jnp.minimum(score, 0.0)
        pos = jnp.maximum(score, 0.0)
        soft = jnp.log(1.0 + jnp.exp2(neg - pos)) * LOG2E
        stay = pos + soft
        if masked:
            row = lax.broadcasted_iota(jnp.int32, (rows_group, 1), 0)
            strip = lax.div(row, piece)
            place = (g * strips + strip) * (2 * tok) + c * tok + x * piece + (row - strip * piece)
            seen = lax.broadcasted_iota(jnp.int32, (rows_group, tok), 1) < place - j * tok
            stay = jnp.where(seen, stay, 0.0)
        stay = stay.astype(BF16)
        suffix = jnp.dot(stay, tri[...], preferred_element_type=F32)
        behind = later[rows]
        whole = jnp.concatenate([behind] * (tok // LANES), axis=1)
        weight = jnp.exp2(neg - soft - suffix - whole)
        if masked:
            weight = jnp.where(seen, weight, 0.0)
        acc[rows] += jnp.dot(weight.astype(BF16), tile, preferred_element_type=F32)
        total = suffix[:, 0:1] + stay[:, 0:1].astype(F32)
        later[rows] = behind + jnp.broadcast_to(total, (rows_group, LANES))

    for low_group in reversed(range(GROUPS)):
        tiles = 2 * strips

        def step(i, carry, low_group=low_group, tiles=tiles):
            j = tiles * (low_group + 1) - 1 - i
            for g in range(low_group, GROUPS):
                tile_step(j, g, g == low_group)
            return carry

        lax.fori_loop(0, tiles, step, 0)
        if low_group:
            serve(3 + GROUPS - 1 - low_group)

    for zs in range(nz):
        rows = acc[zs * piece : (zs + 1) * piece]
        mo[zs] = jnp.where(low(half), swap(rows[:half]), rows[half:]).astype(BF16)
    m2[z] = mo[z]
    for d in order:
        h = zat(d)
        copy = remote(mo.at[h], m2.at[z], m2_s.at[d - 1], m2_r.at[d - 1], sp=h * 2 + c)
        copy.start()
        ends.append(copy)

    own_wo.wait()
    for d in range(1, nx):
        got = wo.at[xat(-d), own_half]
        remote(wo_ref.at[own_half], got, wo_s.at[d - 1], wo_r.at[d - 1], tp=xat(d)).wait_recv()
        copy = remote(got, got, wop_s.at[d - 1], wop_r.at[d - 1], sp=partner)
        copy.start()
        ends.append(copy)
    other_half = pl.ds(pl.multiple_of((1 - c) * share, share), share)
    for d in range(1, nx):
        there = wo.at[xat(-d), other_half]
        remote(there, there, wop_s.at[d - 1], wop_r.at[d - 1], sp=partner).wait_recv()
    for d in order:
        zs = zat(-d)
        remote(mo.at[z], m2.at[zs], m2_s.at[d - 1], m2_r.at[d - 1], sp=zat(d) * 2 + c).wait_recv()
    serve(6)

    top, bottom = [], []
    keep = low(half)
    for p in range(nz // 2):
        a, b = m2[2 * p].astype(F32), m2[2 * p + 1].astype(F32)
        top.append(jnp.where(keep, a, swap(b)).astype(BF16))
        bottom.append(jnp.where(keep, swap(a), b).astype(BF16))
    mixed = jnp.concatenate(
        [jnp.concatenate(top, axis=1), jnp.concatenate(bottom, axis=1)], axis=0
    )
    chunk = min(512, width)
    square = jnp.zeros((piece, 1), F32)
    for n in range(width // chunk):
        cols = slice(n * chunk, (n + 1) * chunk)
        weight = wo[:, :, cols].reshape(nx * wo.shape[1], chunk)
        added = resid_ref[:, cols].astype(F32) + jnp.dot(
            mixed, weight, preferred_element_type=F32
        )
        added = added.astype(BF16)
        state[:, cols] = added
        added = added.astype(F32)
        square += jnp.sum(added * added, axis=1, keepdims=True)
    factor = lax.rsqrt(square / width + EPS)
    mine_rows = pl.ds(pl.multiple_of(HALO + x * piece, HALO), piece)
    ext[mine_rows] = (state[...].astype(F32) * factor * gain_ref[...]).astype(BF16)

    for d in range(1, nx):
        rows = ext.at[mine_rows]
        copy = remote(rows, rows, nx_s.at[d - 1], nx_r.at[d - 1], tp=xat(d))
        copy.start()
        ends.append(copy)

    rim = ext.at[nx * piece : nx * piece + HALO]
    rims = [
        remote(rim, ext.at[0:HALO], ha_s.at[xp], ha_r, sp=after, tp=xp) for xp in range(nx)
    ]

    @pl.when(last_x)
    def _():
        for copy in rims:
            copy.start()

    serve(7)
    serve(8)
    for d in range(1, nx):
        rows = ext.at[pl.ds(pl.multiple_of(HALO + xat(-d) * piece, HALO), piece)]
        remote(rows, rows, nx_s.at[d - 1], nx_r.at[d - 1], tp=xat(d)).wait_recv()
    rims[0].wait_recv()

    @pl.when(sp == 0)
    def _():
        ext[0:HALO] = jnp.zeros((HALO, width), BF16)

    for index in range(nz):
        there = wf.at[slab_rows(zat(-index), 1 - c)]
        remote(there, there, wp_s.at[index], wp_r.at[index], sp=partner).wait_recv()

    chunk = min(256, ff)

    def conv(pre, taps, cols):
        pre = pre.astype(BF16).astype(F32)
        count = taps.shape[0]
        total = taps[0:1, cols] * pre[HALO - count + 1 : HALO - count + 1 + tok]
        for i in range(1, count):
            at = HALO - count + 1 + i
            total = total + taps[i : i + 1, cols] * pre[at : at + tok]
        return total

    for n in range(ff // chunk):
        cols = slice(n * chunk, (n + 1) * chunk)
        gate = jnp.dot(ext[...], wf[:, cols], preferred_element_type=F32)
        value = jnp.dot(
            ext[...], wf[:, ff + n * chunk : ff + (n + 1) * chunk], preferred_element_type=F32
        )
        gate = conv(gate, cg_ref, cols)
        value = conv(value, cv_ref, cols)
        gated[:, cols] = (gate / (1.0 + jnp.exp(-gate)) * value).astype(BF16)

    def rs_copy(d, cols):
        return remote(
            rsb.at[pl.ds(pl.multiple_of(xat(d) * piece, piece), piece), cols],
            rsr.at[d - 1, :, cols], rs_s.at[d - 1], rs_r.at[d - 1], tp=xat(d),
        )

    far_first = sorted(range(1, nx), key=lambda d: -min(d, nx - d))
    for n in range(nz // 2):
        sides = []
        for zz in (2 * n, 2 * n + 1):
            sides.append(
                jnp.concatenate(
                    [
                        wf[
                            (zz * 2 + cc) * slab : (zz * 2 + cc + 1) * slab,
                            2 * ff + j * LANES : 2 * ff + (j + 1) * LANES,
                        ]
                        for cc in range(2)
                        for j in range(blocks)
                    ],
                    axis=0,
                )
            )
        part = jnp.dot(
            gated[...], jnp.concatenate(sides, axis=1), preferred_element_type=F32
        )
        cols = slice(n * 2 * LANES, (n + 1) * 2 * LANES)
        pf[:, cols] = part
        rsb[:, cols] = part.astype(BF16)
        for d in far_first:
            rs_copy(d, cols).start()
    everything = slice(0, width)
    total = state[...].astype(F32) + pf[pl.ds(pl.multiple_of(x * piece, piece), piece)]
    for d in range(1, nx):
        rs_copy(d, everything).wait_recv()
        total = total + rsr[d - 1].astype(F32)
    out_ref[...] = total.astype(BF16)

    for copy in ends:
        copy.wait_send()
    for e in range(1, nx):
        remote(
            s2.at[:, 0:piece], kv.at[:, c, x], s3_s.at[e - 1], s3_r.at[e - 1], tp=xat(e)
        ).wait_send()
        rs_copy(e, everything).wait_send()

    @pl.when(last_x)
    def _():
        for copy in rims:
            copy.wait_send()


def body(*args):
    queries, keys, values, resid, out_weight, gate_weight = args[:6]
    nx, nz = lax.axis_size("tp"), lax.axis_size("sp") // 2
    tok, mix = queries.shape
    piece, width = resid.shape
    ff = gate_weight.shape[1]
    slab = gate_weight.shape[0]
    heads = mix // HEAD
    assert heads * nx == nz
    blocks = ff // 2 // slab
    dims = (nx, nz, heads, tok, piece, width, ff, slab)
    packed = piece + piece // 2
    vmem = pltpu.VMEM
    dma = pltpu.SemaphoreType.DMA
    scratch = [
        vmem((nx, heads, packed, LANES), BF16),
        vmem((nx, heads, packed, LANES), BF16),
        vmem((nz, packed, LANES), BF16),
        vmem((nz, 2, nx, piece, LANES), BF16),
        vmem((nz * piece, LANES), BF16),
        vmem((tok, tok), BF16),
        vmem((nz * piece, LANES), F32),
        vmem((nz * piece, LANES), F32),
        vmem((nz, piece // 2, LANES), BF16),
        vmem((nz, piece // 2, LANES), BF16),
        vmem((nx, out_weight.shape[0], width), BF16),
        vmem((2 * nz * slab, 2 * ff + blocks * LANES), BF16),
        vmem((ff // 2, HEAD), BF16),
        vmem((piece, width), BF16),
        vmem((HALO + tok, width), BF16),
        vmem((tok, ff), BF16),
        vmem((tok, width), BF16),
        vmem((tok, width), F32),
        vmem((nx - 1, piece, width), BF16),
    ]
    sems = [
        dma((nx - 1,)), dma((nx - 1,)),
        dma((nz - 1,)), dma((nz - 1,)),
        dma((nx - 1,)), dma((nx - 1,)),
        dma((nx,)), dma((nx,)),
        dma((nz // 2,)), dma((nz // 2,)),
        dma((nz - 1 - nz // 2,)), dma((nz - 1 - nz // 2,)),
        dma((nz,)), dma((nz,)),
        dma, dma((nx - 1,)), dma((nx - 1,)),
        dma((nx - 1,)), dma((nx - 1,)),
        dma((nz - 1,)), dma((nz - 1,)),
        dma((nx - 1,)), dma((nx - 1,)),
        dma((nx,)), dma,
        dma((nx - 1,)), dma((nx - 1,)),
        dma, dma,
    ]
    in_vmem = pl.BlockSpec(memory_space=pltpu.VMEM)
    specs = [in_vmem] * 11
    specs[4] = pl.BlockSpec(memory_space=pl.ANY)
    args = list(args)
    args[9] = args[9].reshape(1, width)
    return pl.pallas_call(
        functools.partial(kernel, dims),
        out_shape=jax.ShapeDtypeStruct((piece, width), BF16),
        in_specs=specs,
        out_specs=in_vmem,
        scratch_shapes=scratch + sems,
        compiler_params=pltpu.CompilerParams(
            collective_id=0, has_side_effects=True, vmem_limit_bytes=48 * 1024 * 1024
        ),
        name="layer",
    )(*args)


def solution(mesh):
    placed = (
        P(("grp", "sp"), "tp"),
        P(("grp", "sp"), "tp"),
        P(("grp", "sp"), "tp"),
        P(("grp", "sp", "tp"), None),
        P("tp", None),
        P("sp", "tp"),
        P("sp", "tp"),
        P(None, "tp"),
        P(None, "tp"),
        P(),
        P("tp", "sp"),
    )
    return jax.shard_map(
        body, mesh=mesh, in_specs=placed, out_specs=P(("grp", "sp", "tp"), None), check_vma=False
    )
```

```python
import functools
import math

import jax
import jax.numpy as jnp
from jax import lax
from jax.experimental import pallas as pl
from jax.experimental.pallas import tpu as pltpu
from jax.sharding import PartitionSpec as P

HEAD = 64
LANES = 128
EPS = 1e-06
GROUPS = 4
HALO = 16
MESH = pl.DeviceIdType.MESH
F32 = jnp.float32
BF16 = jnp.bfloat16
LOG2E = math.log2(math.e)


def kernel(
    dims,
    q_hbm, k_hbm, v_hbm, resid_hbm, wo_ref, gw_ref, vw_ref, cg_ref, cv_ref, gain_ref, dw_ref,
    out_ref,
    q_ref, k_ref, v_ref, resid_ref, dwn, place, pack, s1, s2, kv, qx, tri, acc, later, mo, m2, wo, wf, dpart, state, ext, gated, rsb, pf, rsr,
    s1_s, s1_r, s2_s, s2_r, s3_s, s3_r, sp_s, sp_r, in_l, cw_s, cw_r, cc_s, cc_r, wp_s, wp_r,
    wo_l, wo_s, wo_r, wop_s, wop_r, m2_s, m2_r, nx_s, nx_r, ha_s, ha_r, rs_s, rs_r, dp_s, dp_r,
):
    nx, nz, heads, tok, piece, width, ff, slab = dims
    half = piece // 2
    down_rows = ff // 2
    blocks = down_rows // slab
    strips = nz // GROUPS
    rows_group = strips * piece
    sp = lax.axis_index("sp")
    x = lax.axis_index("tp")
    z = lax.div(sp, 2)
    c = lax.rem(sp, 2)
    partner = z * 2 + 1 - c
    low = lambda rows: lax.broadcasted_iota(jnp.int32, (rows, LANES), 1) < HEAD
    swap = lambda a: pltpu.roll(a, HEAD, 1)

    def xat(d):
        return lax.rem(x + d + nx, nx)

    def zat(d):
        return lax.rem(z + d + nz, nz)

    def remote(src, dst, send, recv, **where):
        return pltpu.make_async_remote_copy(
            src_ref=src, dst_ref=dst, send_sem=send, recv_sem=recv, device_id=where,
            device_id_type=MESH,
        )

    def slab_rows(zz, cc):
        return pl.ds(pl.multiple_of((zz * 2 + cc) * slab, slab), slab)

    loads = []
    for i, (src, dst) in enumerate(
        (
            (q_hbm, q_ref),
            (k_hbm, k_ref),
            (v_hbm, v_ref),
            (dw_ref.at[:, pl.ds(pl.multiple_of(c * down_rows, LANES), down_rows)], dwn),
            (gw_ref, wf.at[slab_rows(z, c), 0:ff]),
            (vw_ref, wf.at[slab_rows(z, c), ff : 2 * ff]),
            (resid_hbm, resid_ref),
        )
    ):
        loads.append(pltpu.make_async_copy(src, dst, in_l.at[i]))
        loads[-1].start()
    own_wo = pltpu.make_async_copy(wo_ref, wo.at[x], wo_l)
    own_wo.start()
    for load in loads[:3]:
        load.wait()

    for xp in range(nx):
        at = xp * piece
        for p in range(heads // 2):
            cols = slice(p * LANES, (p + 1) * LANES)
            kk = k_ref[at : at + piece, cols].astype(F32)
            vv = v_ref[at : at + piece, cols].astype(F32)
            qq = q_ref[at : at + piece, cols].astype(F32)
            qr = swap(qq)
            keep = low(piece)
            pack[xp, 2 * p, 0:piece] = jnp.where(keep, kk, swap(vv)).astype(BF16)
            pack[xp, 2 * p + 1, 0:piece] = jnp.where(keep, swap(kk), vv).astype(BF16)
            keep = low(half)
            pack[xp, 2 * p, piece:] = jnp.where(keep, qq[:half], qr[half:]).astype(BF16)
            pack[xp, 2 * p + 1, piece:] = jnp.where(keep, qr[:half], qq[half:]).astype(BF16)
    s1[x] = pack[x]

    barrier = pltpu.get_barrier_semaphore()
    last_x = x == nx - 1
    before = lax.rem(sp + 2 * nz - 1, 2 * nz)
    after = lax.rem(sp + 1, 2 * nz)

    def greet(**where):
        pl.semaphore_signal(barrier, inc=1, device_id=where, device_id_type=MESH)

    for d in range(1, nx):
        greet(tp=xat(d))
    for d in range(1, nz):
        greet(sp=zat(d) * 2 + c)
    greet(sp=partner)
    greet(sp=before, tp=nx - 1)

    @pl.when(last_x)
    def _():
        for xp in range(nx):
            greet(sp=after, tp=xp)

    pl.semaphore_wait(barrier, nx - 1 + nz - 1 + 2 + jnp.where(last_x, nx, 0))

    ends = []
    for d in range(1, nx):
        copy = remote(pack.at[xat(d)], s1.at[x], s1_s.at[d - 1], s1_r.at[d - 1], tp=xat(d))
        copy.start()
        ends.append(copy)
    down_part = remote(
        dw_ref.at[:, pl.ds(pl.multiple_of((1 - c) * down_rows, LANES), down_rows)], dpart, dp_s,
        dp_r, sp=partner,
    )
    down_part.start()
    ends.append(down_part)
    share = wo_ref.shape[0] // 2
    own_half = pl.ds(pl.multiple_of(c * share, share), share)
    wo_parts = nz
    wo_cols = width // wo_parts

    def send_wo(part):
        cols = slice(part * wo_cols, (part + 1) * wo_cols)
        for d in range(1, nx):
            remote(
                wo_ref.at[own_half, cols], wo.at[x, own_half, cols], wo_s.at[d - 1],
                wo_r.at[d - 1], tp=xat(d),
            ).start()

    down_part.wait_recv()
    for load in loads[3:6]:
        load.wait()
    mine = dwn[...].astype(F32)
    other = dpart[...].astype(F32)
    first = c == 0
    row = lax.broadcasted_iota(jnp.int32, (HEAD, LANES), 0)
    col = lax.broadcasted_iota(jnp.int32, (HEAD, LANES), 1)
    turn = (((0,), (0,)), ((), ()))
    both = lax.dot_general(
        jnp.where(first, mine, other).astype(BF16), (row == col).astype(BF16), turn,
        preferred_element_type=F32,
    ) + lax.dot_general(
        jnp.where(first, other, mine).astype(BF16), (row + HEAD == col).astype(BF16), turn,
        preferred_element_type=F32,
    )
    both = both.astype(BF16)
    for j in range(blocks):
        wf[slab_rows(z, c), 2 * ff + j * LANES : 2 * ff + (j + 1) * LANES] = both[
            j * slab : (j + 1) * slab
        ]
    hops = (nz // 2, nz - 1 - nz // 2)
    lanes = (slice(0, 2 * ff), slice(2 * ff, 2 * ff + blocks * LANES))

    def ring(way, kind, step):
        origin = zat(-step) if way == 0 else zat(step)
        part = wf.at[slab_rows(origin, c), lanes[kind]]
        sends, recvs = ((cw_s, cw_r), (cc_s, cc_r))[way]
        to = zat(1) if way == 0 else zat(-1)
        return remote(part, part, sends.at[kind, step], recvs.at[kind, step], sp=to * 2 + c)

    def come(way, kind, step):
        origin = zat(-step) if way == 0 else zat(step)
        part = wf.at[slab_rows(origin, c), lanes[kind]]
        sends, recvs = ((cw_s, cw_r), (cc_s, cc_r))[way]
        to = zat(1) if way == 0 else zat(-1)
        return remote(
            part, part, sends.at[kind, step - 1], recvs.at[kind, step - 1], sp=to * 2 + c
        )

    def begin(copy):
        copy.start()
        ends.append(copy)

    def send_across(origin, kind, index):
        part = wf.at[slab_rows(origin, c), lanes[kind]]
        begin(remote(part, part, wp_s.at[kind, index], wp_r.at[kind, index], sp=partner))

    for kind in range(2):
        for way in range(2):
            begin(ring(way, kind, 0))
    for kind in range(2):
        send_across(z, kind, 0)

    def serve(step):
        for kind in range(2):
            at = step - kind
            for way in range(2):
                if 1 <= at <= hops[way]:
                    come(way, kind, at).wait_recv()
                    if at < hops[way]:
                        begin(ring(way, kind, at))
                    send_across(
                        zat(-at) if way == 0 else zat(at), kind, at if way == 0 else nz - at
                    )

    for d in range(1, nx):
        remote(
            pack.at[x], s1.at[xat(-d)], s1_s.at[d - 1], s1_r.at[d - 1], tp=xat(d)
        ).wait_recv()
    s2[z] = s1[lax.div(z, heads), lax.rem(z, heads)]
    order = sorted(range(1, nz), key=lambda d: (min(d, nz - d), d))
    for d in order:
        h = zat(d)
        copy = remote(
            s1.at[lax.div(h, heads), lax.rem(h, heads)], s2.at[z], s2_s.at[d - 1], s2_r.at[d - 1],
            sp=h * 2 + c,
        )
        copy.start()
        ends.append(copy)

    r = lax.broadcasted_iota(jnp.int32, (tok, tok), 0)
    s = lax.broadcasted_iota(jnp.int32, (tok, tok), 1)
    tri[...] = (r > s).astype(BF16)
    row = lax.broadcasted_iota(jnp.int32, (nz * piece, LANES), 0)
    strip = lax.div(row, piece)
    place[...] = strip * (2 * tok - piece) + row + c * tok + x * piece
    acc[...] = jnp.zeros_like(acc)
    later[...] = jnp.zeros_like(later)
    for number, d in enumerate([0] + order):
        zs = zat(-d)
        if number < wo_parts // 2:
            send_wo(number)
        if d:
            remote(
                s2.at[z], s2.at[zs], s2_s.at[d - 1], s2_r.at[d - 1], sp=zat(d) * 2 + c
            ).wait_recv()
        kv[zs, c, x] = s2[zs, 0:piece]
        for e in range(1, nx):
            remote(
                s2.at[zs, 0:piece], kv.at[zs, c, x], s3_s.at[e - 1], s3_r.at[e - 1], tp=xat(e)
            ).start()
        packed = s2[zs, piece:].astype(F32)
        keep = low(half)
        at = pl.multiple_of(zs * piece, piece)
        qx[pl.ds(at, half)] = jnp.where(keep, packed, 0.0).astype(BF16)
        qx[pl.ds(pl.multiple_of(at + half, half), half)] = jnp.where(
            keep, swap(packed), 0.0
        ).astype(BF16)
    across = remote(
        s2.at[:, 0:piece], kv.at[:, c, x], sp_s.at[0], sp_r.at[0], sp=partner
    )
    across.start()
    ends.append(across)
    for part in range(wo_parts // 2, wo_parts):
        send_wo(part)
    serve(1)
    for e in (1, nx - 1) + tuple(range(2, nx - 1)) if nx > 2 else (1,):
        source = xat(-e)
        got = kv.at[:, c, source]
        remote(
            s2.at[:, 0:piece], got, s3_s.at[e - 1], s3_r.at[e - 1], tp=xat(e)
        ).wait_recv()
        across = remote(got, got, sp_s.at[e], sp_r.at[e], sp=partner)
        across.start()
        ends.append(across)
    for e in range(nx):
        there = kv.at[:, 1 - c, xat(-e)]
        remote(there, there, sp_s.at[e], sp_r.at[e], sp=partner).wait_recv()
    serve(2)

    scale = LOG2E / math.sqrt(HEAD)

    def group_rows(g):
        return slice(g * rows_group, (g + 1) * rows_group)

    def chances(j, g, masked):
        tile = kv[lax.div(j, 2), lax.rem(j, 2)].reshape(tok, LANES)
        score = lax.dot_general(
            qx[group_rows(g)], tile, (((1,), (1,)), ((), ())), preferred_element_type=F32
        ) * scale
        neg = jnp.minimum(score, 0.0)
        pos = jnp.maximum(score, 0.0)
        soft = jnp.log2(1.0 + jnp.exp2(neg - pos))
        stay = pos + soft
        seen = None
        if masked:
            where = jnp.concatenate([place[group_rows(g)]] * (tok // LANES), axis=1)
            seen = lax.broadcasted_iota(jnp.int32, (rows_group, tok), 1) < where - j * tok
            stay = jnp.where(seen, stay, 0.0)
        return tile, neg - soft, stay.astype(BF16), seen

    def weights(tile, go, stay, seen):
        suffix = jnp.dot(stay, tri[...], preferred_element_type=F32)
        weight = jnp.exp2(go - suffix)
        if seen is not None:
            weight = jnp.where(seen, weight, 0.0)
        return tile, weight.astype(BF16), suffix[:, 0:1] + stay[:, 0:1].astype(F32)

    def gather(g, tile, weight, total):
        rows = group_rows(g)
        behind = later[rows]
        acc[rows] += jnp.exp2(-behind) * jnp.dot(weight, tile, preferred_element_type=F32)
        later[rows] = behind + jnp.broadcast_to(total, (rows_group, LANES))

    for low_group in reversed(range(GROUPS)):
        tiles = 2 * strips
        active = list(range(low_group, GROUPS))
        unroll = min(tiles, 4 if len(active) == 1 else 2)

        def step(i, carry, low_group=low_group, active=active, unroll=unroll):
            tasks = [
                (tiles * (low_group + 1) - 1 - i * unroll - u, g)
                for u in range(unroll)
                for g in active
            ]
            held = {}
            for t in range(len(tasks) + 2):
                if t < len(tasks):
                    j, g = tasks[t]
                    held[t] = chances(j, g, g == low_group)
                if 1 <= t <= len(tasks):
                    held[t - 1] = weights(*held[t - 1])
                if t >= 2:
                    gather(tasks[t - 2][1], *held.pop(t - 2))
            return carry

        lax.fori_loop(0, tiles // unroll, step, 0)
        if low_group != GROUPS - 1:
            serve(3 + GROUPS - 2 - low_group)

    for zs in range(nz):
        rows = acc[zs * piece : (zs + 1) * piece]
        mo[zs] = jnp.where(low(half), swap(rows[:half]), rows[half:]).astype(BF16)
    m2[z] = mo[z]
    for d in order:
        h = zat(d)
        copy = remote(mo.at[h], m2.at[z], m2_s.at[d - 1], m2_r.at[d - 1], sp=h * 2 + c)
        copy.start()
        ends.append(copy)

    serve(6)

    own_wo.wait()
    for d in range(1, nx):
        got = wo.at[xat(-d), own_half]
        remote(wo_ref.at[own_half], got, wo_s.at[d - 1], wo_r.at[d - 1], tp=xat(d)).wait_recv()
        copy = remote(got, got, wop_s.at[d - 1], wop_r.at[d - 1], sp=partner)
        copy.start()
        ends.append(copy)
    other_half = pl.ds(pl.multiple_of((1 - c) * share, share), share)
    for d in range(1, nx):
        there = wo.at[xat(-d), other_half]
        remote(there, there, wop_s.at[d - 1], wop_r.at[d - 1], sp=partner).wait_recv()
    for d in order:
        zs = zat(-d)
        remote(mo.at[z], m2.at[zs], m2_s.at[d - 1], m2_r.at[d - 1], sp=zat(d) * 2 + c).wait_recv()
    serve(7)

    top, bottom = [], []
    keep = low(half)
    for p in range(nz // 2):
        a, b = m2[2 * p].astype(F32), m2[2 * p + 1].astype(F32)
        top.append(jnp.where(keep, a, swap(b)).astype(BF16))
        bottom.append(jnp.where(keep, swap(a), b).astype(BF16))
    mixed = jnp.concatenate(
        [jnp.concatenate(top, axis=1), jnp.concatenate(bottom, axis=1)], axis=0
    )
    loads[6].wait()
    chunk = min(512, width)
    square = jnp.zeros((piece, 1), F32)
    for n in range(width // chunk):
        cols = slice(n * chunk, (n + 1) * chunk)
        weight = wo[:, :, cols].reshape(nx * wo.shape[1], chunk)
        added = resid_ref[:, cols].astype(F32) + jnp.dot(
            mixed, weight, preferred_element_type=F32
        )
        added = added.astype(BF16)
        state[:, cols] = added
        added = added.astype(F32)
        square += jnp.sum(added * added, axis=1, keepdims=True)
    factor = lax.rsqrt(square / width + EPS)
    mine_rows = pl.ds(pl.multiple_of(HALO + x * piece, HALO), piece)
    ext[mine_rows] = (state[...].astype(F32) * factor * gain_ref[...]).astype(BF16)

    for d in range(1, nx):
        rows = ext.at[mine_rows]
        copy = remote(rows, rows, nx_s.at[d - 1], nx_r.at[d - 1], tp=xat(d))
        copy.start()
        ends.append(copy)

    rim = ext.at[nx * piece : nx * piece + HALO]
    rims = [
        remote(rim, ext.at[0:HALO], ha_s.at[xp], ha_r, sp=after, tp=xp) for xp in range(nx)
    ]

    @pl.when(last_x)
    def _():
        for copy in rims:
            copy.start()

    serve(8)
    serve(9)
    for d in range(1, nx):
        rows = ext.at[pl.ds(pl.multiple_of(HALO + xat(-d) * piece, HALO), piece)]
        remote(rows, rows, nx_s.at[d - 1], nx_r.at[d - 1], tp=xat(d)).wait_recv()
    rims[0].wait_recv()

    @pl.when(sp == 0)
    def _():
        ext[0:HALO] = jnp.zeros((HALO, width), BF16)

    def all_across(kind):
        for index in range(nz):
            there = wf.at[slab_rows(zat(-index), 1 - c), lanes[kind]]
            remote(
                there, there, wp_s.at[kind, index], wp_r.at[kind, index], sp=partner
            ).wait_recv()

    all_across(0)

    chunk = min(256, ff)

    def conv(pre, taps, cols):
        pre = pre.astype(BF16).astype(F32)
        count = taps.shape[0]
        total = taps[0:1, cols] * pre[HALO - count + 1 : HALO - count + 1 + tok]
        for i in range(1, count):
            at = HALO - count + 1 + i
            total = total + taps[i : i + 1, cols] * pre[at : at + tok]
        return total

    for n in range(ff // chunk):
        cols = slice(n * chunk, (n + 1) * chunk)
        gate = jnp.dot(ext[...], wf[:, cols], preferred_element_type=F32)
        value = jnp.dot(
            ext[...], wf[:, ff + n * chunk : ff + (n + 1) * chunk], preferred_element_type=F32
        )
        gate = conv(gate, cg_ref, cols)
        value = conv(value, cv_ref, cols)
        gated[:, cols] = (gate / (1.0 + jnp.exp(-gate)) * value).astype(BF16)

    def rs_copy(d, cols):
        return remote(
            rsb.at[pl.ds(pl.multiple_of(xat(d) * piece, piece), piece), cols],
            rsr.at[d - 1, :, cols], rs_s.at[d - 1], rs_r.at[d - 1], tp=xat(d),
        )

    all_across(1)
    far_first = sorted(range(1, nx), key=lambda d: -min(d, nx - d))
    for n in range(nz // 2):
        sides = []
        for zz in (2 * n, 2 * n + 1):
            sides.append(
                jnp.concatenate(
                    [
                        wf[
                            (zz * 2 + cc) * slab : (zz * 2 + cc + 1) * slab,
                            2 * ff + j * LANES : 2 * ff + (j + 1) * LANES,
                        ]
                        for cc in range(2)
                        for j in range(blocks)
                    ],
                    axis=0,
                )
            )
        part = jnp.dot(
            gated[...], jnp.concatenate(sides, axis=1), preferred_element_type=F32
        )
        cols = slice(n * 2 * LANES, (n + 1) * 2 * LANES)
        pf[:, cols] = part
        rsb[:, cols] = part.astype(BF16)
        for d in far_first:
            rs_copy(d, cols).start()
    everything = slice(0, width)
    total = state[...].astype(F32) + pf[pl.ds(pl.multiple_of(x * piece, piece), piece)]
    for d in range(1, nx):
        rs_copy(d, everything).wait_recv()
        total = total + rsr[d - 1].astype(F32)
    out_ref[...] = total.astype(BF16)

    for copy in ends:
        copy.wait_send()
    for e in range(1, nx):
        remote(
            s2.at[:, 0:piece], kv.at[:, c, x], s3_s.at[e - 1], s3_r.at[e - 1], tp=xat(e)
        ).wait_send()
        rs_copy(e, everything).wait_send()
        remote(
            wo_ref.at[own_half], wo.at[x, own_half], wo_s.at[e - 1], wo_r.at[e - 1], tp=xat(e)
        ).wait_send()

    @pl.when(last_x)
    def _():
        for copy in rims:
            copy.wait_send()


def body(*args):
    queries, keys, values, resid, out_weight, gate_weight = args[:6]
    nx, nz = lax.axis_size("tp"), lax.axis_size("sp") // 2
    tok, mix = queries.shape
    piece, width = resid.shape
    ff = gate_weight.shape[1]
    slab = gate_weight.shape[0]
    heads = mix // HEAD
    assert heads * nx == nz
    blocks = ff // 2 // slab
    dims = (nx, nz, heads, tok, piece, width, ff, slab)
    packed = piece + piece // 2
    vmem = pltpu.VMEM
    dma = pltpu.SemaphoreType.DMA
    scratch = [
        vmem((tok, mix), BF16),
        vmem((tok, mix), BF16),
        vmem((tok, mix), BF16),
        vmem((piece, width), BF16),
        vmem((HEAD, ff // 2), BF16),
        vmem((nz * piece, LANES), jnp.int32),
        vmem((nx, heads, packed, LANES), BF16),
        vmem((nx, heads, packed, LANES), BF16),
        vmem((nz, packed, LANES), BF16),
        vmem((nz, 2, nx, piece, LANES), BF16),
        vmem((nz * piece, LANES), BF16),
        vmem((tok, tok), BF16),
        vmem((nz * piece, LANES), F32),
        vmem((nz * piece, LANES), F32),
        vmem((nz, piece // 2, LANES), BF16),
        vmem((nz, piece // 2, LANES), BF16),
        vmem((nx, out_weight.shape[0], width), BF16),
        vmem((2 * nz * slab, 2 * ff + blocks * LANES), BF16),
        vmem((HEAD, ff // 2), BF16),
        vmem((piece, width), BF16),
        vmem((HALO + tok, width), BF16),
        vmem((tok, ff), BF16),
        vmem((tok, width), BF16),
        vmem((tok, width), F32),
        vmem((nx - 1, piece, width), BF16),
    ]
    sems = [
        dma((nx - 1,)), dma((nx - 1,)),
        dma((nz - 1,)), dma((nz - 1,)),
        dma((nx - 1,)), dma((nx - 1,)),
        dma((nx,)), dma((nx,)),
        dma((7,)),
        dma((2, nz // 2)), dma((2, nz // 2)),
        dma((2, nz // 2)), dma((2, nz // 2)),
        dma((2, nz)), dma((2, nz)),
        dma, dma((nx - 1,)), dma((nx - 1,)),
        dma((nx - 1,)), dma((nx - 1,)),
        dma((nz - 1,)), dma((nz - 1,)),
        dma((nx - 1,)), dma((nx - 1,)),
        dma((nx,)), dma,
        dma((nx - 1,)), dma((nx - 1,)),
        dma, dma,
    ]
    in_vmem = pl.BlockSpec(memory_space=pltpu.VMEM)
    anywhere = pl.BlockSpec(memory_space=pl.ANY)
    specs = [anywhere] * 7 + [in_vmem] * 3 + [anywhere]
    args = list(args)
    args[9] = args[9].reshape(1, width)
    args[10] = args[10].T
    return pl.pallas_call(
        functools.partial(kernel, dims),
        out_shape=jax.ShapeDtypeStruct((piece, width), BF16),
        in_specs=specs,
        out_specs=in_vmem,
        scratch_shapes=scratch + sems,
        compiler_params=pltpu.CompilerParams(
            collective_id=0, has_side_effects=True, vmem_limit_bytes=67043328
        ),
        name="layer",
    )(*args)


def solution(mesh):
    placed = (
        P(("grp", "sp"), "tp"),
        P(("grp", "sp"), "tp"),
        P(("grp", "sp"), "tp"),
        P(("grp", "sp", "tp"), None),
        P("tp", None),
        P("sp", "tp"),
        P("sp", "tp"),
        P(None, "tp"),
        P(None, "tp"),
        P(),
        P("tp", "sp"),
    )
    return jax.shard_map(
        body, mesh=mesh, in_specs=placed, out_specs=P(("grp", "sp", "tp"), None), check_vma=False
    )
```

```python
import functools
import math

import jax
import jax.numpy as jnp
from jax import lax
from jax.experimental import pallas as pl
from jax.experimental.pallas import tpu as pltpu
from jax.sharding import PartitionSpec as P

HEAD = 64
LANES = 128
EPS = 1e-06
GROUPS = 4
HALO = 16
MESH = pl.DeviceIdType.MESH
F32 = jnp.float32
BF16 = jnp.bfloat16
LOG2E = math.log2(math.e)


def kernel(
    dims,
    q_hbm, k_hbm, v_hbm, resid_hbm, wo_ref, gw_ref, vw_ref, cg_ref, cv_ref, gain_ref, dw_ref,
    out_ref,
    q_ref, k_ref, v_ref, resid_ref, dwn, place, pack, s1, s2, kv, qx, tri, acc, later, mo, m2, wo, wf, dpart, state, ext, gated, rsb, pf, rsr,
    s1_s, s1_r, s2_s, s2_r, s3_s, s3_r, sp_s, sp_r, in_l, cw_s, cw_r, cc_s, cc_r, wp_s, wp_r, wy_s, wy_r,
    wo_l, wo_s, wo_r, wop_s, wop_r, m2_s, m2_r, nx_s, nx_r, ha_s, ha_r, rs_s, rs_r, dp_s, dp_r,
):
    nx, nz, heads, tok, piece, width, ff, slab = dims
    half = piece // 2
    down_rows = ff // 2
    blocks = down_rows // slab
    strips = nz // GROUPS
    rows_group = strips * piece
    sp = lax.axis_index("sp")
    x = lax.axis_index("tp")
    z = lax.div(sp, 2)
    c = lax.rem(sp, 2)
    partner = z * 2 + 1 - c
    group = lax.axis_index("grp")
    side = lax.rem(group, 2)
    twin = group + 1 - 2 * side
    low = lambda rows: lax.broadcasted_iota(jnp.int32, (rows, LANES), 1) < HEAD
    swap = lambda a: pltpu.roll(a, HEAD, 1)

    def xat(d):
        return lax.rem(x + d + nx, nx)

    def zat(d):
        return lax.rem(z + d + nz, nz)

    def remote(src, dst, send, recv, **where):
        return pltpu.make_async_remote_copy(
            src_ref=src, dst_ref=dst, send_sem=send, recv_sem=recv, device_id=where,
            device_id_type=MESH,
        )

    def slab_rows(zz, cc):
        return pl.ds(pl.multiple_of((zz * 2 + cc) * slab, slab), slab)

    loads = []
    for i, (src, dst) in enumerate(
        (
            (q_hbm, q_ref),
            (k_hbm, k_ref),
            (v_hbm, v_ref),
            (dw_ref.at[:, pl.ds(pl.multiple_of(c * down_rows, LANES), down_rows)], dwn),
            (gw_ref, wf.at[slab_rows(z, c), 0:ff]),
            (vw_ref, wf.at[slab_rows(z, c), ff : 2 * ff]),
            (resid_hbm, resid_ref),
        )
    ):
        loads.append(pltpu.make_async_copy(src, dst, in_l.at[i]))
        loads[-1].start()
    own_wo = pltpu.make_async_copy(wo_ref, wo.at[x], wo_l)
    own_wo.start()
    for load in loads[:3]:
        load.wait()

    for xp in range(nx):
        at = xp * piece
        for p in range(heads // 2):
            cols = slice(p * LANES, (p + 1) * LANES)
            kk = k_ref[at : at + piece, cols].astype(F32)
            vv = v_ref[at : at + piece, cols].astype(F32)
            qq = q_ref[at : at + piece, cols].astype(F32)
            qr = swap(qq)
            keep = low(piece)
            pack[xp, 2 * p, 0:piece] = jnp.where(keep, kk, swap(vv)).astype(BF16)
            pack[xp, 2 * p + 1, 0:piece] = jnp.where(keep, swap(kk), vv).astype(BF16)
            keep = low(half)
            pack[xp, 2 * p, piece:] = jnp.where(keep, qq[:half], qr[half:]).astype(BF16)
            pack[xp, 2 * p + 1, piece:] = jnp.where(keep, qr[:half], qq[half:]).astype(BF16)
    s1[x] = pack[x]

    barrier = pltpu.get_barrier_semaphore()
    last_x = x == nx - 1
    before = lax.rem(sp + 2 * nz - 1, 2 * nz)
    after = lax.rem(sp + 1, 2 * nz)

    def greet(**where):
        pl.semaphore_signal(barrier, inc=1, device_id=where, device_id_type=MESH)

    for d in range(1, nx):
        greet(tp=xat(d))
    for d in range(1, nz):
        greet(sp=zat(d) * 2 + c)
    greet(sp=partner)
    greet(grp=twin)
    greet(sp=before, tp=nx - 1)

    @pl.when(last_x)
    def _():
        for xp in range(nx):
            greet(sp=after, tp=xp)

    pl.semaphore_wait(barrier, nx - 1 + nz - 1 + 3 + jnp.where(last_x, nx, 0))

    ends = []
    for d in range(1, nx):
        copy = remote(pack.at[xat(d)], s1.at[x], s1_s.at[d - 1], s1_r.at[d - 1], tp=xat(d))
        copy.start()
        ends.append(copy)
    down_part = remote(
        dw_ref.at[:, pl.ds(pl.multiple_of((1 - c) * down_rows, LANES), down_rows)], dpart, dp_s,
        dp_r, sp=partner,
    )
    down_part.start()
    ends.append(down_part)
    share = wo_ref.shape[0] // 2
    own_half = pl.ds(pl.multiple_of(c * share, share), share)
    wo_parts = nz
    wo_cols = width // wo_parts

    def send_wo(part):
        cols = slice(part * wo_cols, (part + 1) * wo_cols)
        for d in range(1, nx):
            remote(
                wo_ref.at[own_half, cols], wo.at[x, own_half, cols], wo_s.at[d - 1],
                wo_r.at[d - 1], tp=xat(d),
            ).start()

    down_part.wait_recv()
    for load in loads[3:6]:
        load.wait()
    mine = dwn[...].astype(F32)
    other = dpart[...].astype(F32)
    first = c == 0
    row = lax.broadcasted_iota(jnp.int32, (HEAD, LANES), 0)
    col = lax.broadcasted_iota(jnp.int32, (HEAD, LANES), 1)
    turn = (((0,), (0,)), ((), ()))
    both = lax.dot_general(
        jnp.where(first, mine, other).astype(BF16), (row == col).astype(BF16), turn,
        preferred_element_type=F32,
    ) + lax.dot_general(
        jnp.where(first, other, mine).astype(BF16), (row + HEAD == col).astype(BF16), turn,
        preferred_element_type=F32,
    )
    both = both.astype(BF16)
    for j in range(blocks):
        wf[slab_rows(z, c), 2 * ff + j * LANES : 2 * ff + (j + 1) * LANES] = both[
            j * slab : (j + 1) * slab
        ]
    hops = (nz // 2, nz - 1 - nz // 2)
    lanes = (
        pl.ds(pl.multiple_of(side * ff, LANES), ff),
        pl.ds(2 * ff, blocks * LANES),
        pl.ds(pl.multiple_of((1 - side) * ff, LANES), ff),
    )

    def slab_part(origin, kind, core=c):
        return wf.at[slab_rows(origin, core), lanes[kind]]

    def from_hops(way, step):
        return zat(-step) if way == 0 else zat(step)

    def ring(way, kind, step, sem):
        part = slab_part(from_hops(way, step), kind)
        sends, recvs = ((cw_s, cw_r), (cc_s, cc_r))[way]
        to = zat(1) if way == 0 else zat(-1)
        return remote(part, part, sends.at[kind, sem], recvs.at[kind, sem], sp=to * 2 + c)

    def across(origin, kind, index, core=c):
        part = slab_part(origin, kind, core)
        return remote(part, part, wp_s.at[kind, index], wp_r.at[kind, index], sp=partner)

    def twin_copy(origin, index, kind=0):
        part = slab_part(origin, kind)
        return remote(part, part, wy_s.at[index], wy_r.at[index], grp=twin)

    def begin(copy):
        copy.start()
        ends.append(copy)

    for kind in range(2):
        for way in range(2):
            begin(ring(way, kind, 0, 0))
    for kind in range(3):
        begin(across(z, kind, 0))

    def serve(step):
        for way in range(2):
            if step <= hops[way]:
                origin, index = from_hops(way, step), step if way == 0 else nz - step
                ring(way, 0, step, step - 1).wait_recv()
                if step < hops[way]:
                    begin(ring(way, 0, step, step))
                begin(twin_copy(origin, index))
                begin(across(origin, 0, index))
        at = step - 1
        for way in range(2):
            if 1 <= at <= hops[way]:
                origin, index = from_hops(way, at), at if way == 0 else nz - at
                ring(way, 1, at, at - 1).wait_recv()
                if at < hops[way]:
                    begin(ring(way, 1, at, at))
                begin(across(origin, 1, index))
                twin_copy(origin, index, 2).wait_recv()
                begin(across(origin, 2, index))

    order = sorted(range(1, nz), key=lambda d: (-min(d, nz - d), d))
    for e in range(1, nx):
        remote(
            pack.at[x], s1.at[xat(-e)], s1_s.at[e - 1], s1_r.at[e - 1], tp=xat(e)
        ).wait_recv()
    s2[z] = s1[lax.div(z, heads), lax.rem(z, heads)]
    for d in order:
        h = zat(d)
        begin(
            remote(
                s1.at[lax.div(h, heads), lax.rem(h, heads)], s2.at[z], s2_s.at[d - 1],
                s2_r.at[d - 1], sp=h * 2 + c,
            )
        )

    r = lax.broadcasted_iota(jnp.int32, (tok, tok), 0)
    s = lax.broadcasted_iota(jnp.int32, (tok, tok), 1)
    tri[...] = (r > s).astype(BF16)
    row = lax.broadcasted_iota(jnp.int32, (nz * piece, LANES), 0)
    strip = lax.div(row, piece)
    place[...] = strip * (2 * tok - piece) + row + c * tok + x * piece
    scale = LOG2E / math.sqrt(HEAD)
    acc[...] = jnp.zeros_like(acc)
    later[...] = jnp.zeros_like(later)
    for d in [0] + order:
        zs = zat(-d)
        if d:
            remote(
                s2.at[z], s2.at[zs], s2_s.at[d - 1], s2_r.at[d - 1], sp=zat(d) * 2 + c
            ).wait_recv()
        kv[zs, c, x] = s2[zs, 0:piece]
        for e in range(1, nx):
            remote(
                s2.at[zs, 0:piece], kv.at[zs, c, x], s3_s.at[e - 1], s3_r.at[e - 1], tp=xat(e)
            ).start()
        packed = s2[zs, piece:].astype(F32)
        keep = low(half)
        at = pl.multiple_of(zs * piece, piece)
        qx[pl.ds(at, half)] = jnp.where(keep, packed, 0.0).astype(BF16)
        qx[pl.ds(pl.multiple_of(at + half, half), half)] = jnp.where(
            keep, swap(packed), 0.0
        ).astype(BF16)
    begin(
        remote(s2.at[:, 0:piece], kv.at[:, c, x], sp_s.at[0], sp_r.at[0], sp=partner)
    )
    for part in range(wo_parts):
        send_wo(part)
    serve(1)
    for e in (1, nx - 1) + tuple(range(2, nx - 1)) if nx > 2 else (1,):
        source = xat(-e)
        got = kv.at[:, c, source]
        remote(
            s2.at[:, 0:piece], got, s3_s.at[e - 1], s3_r.at[e - 1], tp=xat(e)
        ).wait_recv()
        begin(remote(got, got, sp_s.at[e], sp_r.at[e], sp=partner))
    for e in range(nx):
        there = kv.at[:, 1 - c, xat(-e)]
        remote(there, there, sp_s.at[e], sp_r.at[e], sp=partner).wait_recv()
    serve(2)

    tiles = 2 * strips

    def chances(j, rows, masked):
        tile = kv[lax.div(j, 2), lax.rem(j, 2)].reshape(tok, LANES)
        score = lax.dot_general(
            qx[rows], tile, (((1,), (1,)), ((), ())), preferred_element_type=F32
        ) * scale
        neg = jnp.minimum(score, 0.0)
        pos = jnp.maximum(score, 0.0)
        soft = jnp.log2(1.0 + jnp.exp2(neg - pos))
        stay = pos + soft
        seen = None
        if masked:
            where = jnp.concatenate([place[rows]] * (tok // LANES), axis=1)
            seen = lax.broadcasted_iota(jnp.int32, (rows_group, tok), 1) < where - j * tok
            stay = jnp.where(seen, stay, 0.0)
        return tile, neg - soft, stay.astype(BF16), seen

    def weights(tile, go, stay, seen):
        suffix = jnp.dot(stay, tri[...], preferred_element_type=F32)
        weight = jnp.exp2(go - suffix)
        if seen is not None:
            weight = jnp.where(seen, weight, 0.0)
        return tile, weight.astype(BF16), suffix[:, 0:1] + stay[:, 0:1].astype(F32)

    def gather(rows, tile, weight, total):
        behind = later[rows]
        acc[rows] += jnp.exp2(behind) * jnp.dot(weight, tile, preferred_element_type=F32)
        later[rows] = behind - jnp.broadcast_to(total, behind.shape)

    def stretch(low_group, active, unroll):
        unroll = min(tiles, unroll)

        def step(i, carry):
            tasks = [
                (tiles * (low_group + 1) - 1 - i * unroll - u, g)
                for u in range(unroll)
                for g in active
            ]
            held = {}
            for t in range(len(tasks) + 2):
                if t < len(tasks):
                    j, g = tasks[t]
                    held[t] = chances(j, group_rows(g), g == low_group)
                if 1 <= t <= len(tasks):
                    held[t - 1] = weights(*held[t - 1])
                if t >= 2:
                    gather(group_rows(tasks[t - 2][1]), *held.pop(t - 2))
            return carry

        lax.fori_loop(0, tiles // unroll, step, 0)

    def group_rows(g):
        return slice(g * rows_group, (g + 1) * rows_group)

    def send_rows(g):
        for zs in range(g * strips, (g + 1) * strips):
            rows = acc[zs * piece : (zs + 1) * piece]
            mo[zs] = jnp.where(low(half), swap(rows[:half]), rows[half:]).astype(BF16)
        for zs in range(g * strips, (g + 1) * strips):

            @pl.when(z == zs)
            def _():
                m2[zs] = mo[zs]

            @pl.when(z != zs)
            def _():
                d = lax.rem(zs - z + nz, nz) - 1
                remote(mo.at[zs], m2.at[z], m2_s.at[d], m2_r.at[d], sp=zs * 2 + c).start()

    stretch(3, (3,), 4)
    stretch(2, (2, 3), 2)
    serve(3)
    stretch(1, (1, 2, 3), 2)
    serve(4)
    stretch(0, (2, 3), 2)
    send_rows(3)
    send_rows(2)
    stretch(0, (0, 1), 2)
    send_rows(1)
    send_rows(0)

    own_wo.wait()
    for d in range(1, nx):
        got = wo.at[xat(-d), own_half]
        remote(wo_ref.at[own_half], got, wo_s.at[d - 1], wo_r.at[d - 1], tp=xat(d)).wait_recv()
        copy = remote(got, got, wop_s.at[d - 1], wop_r.at[d - 1], sp=partner)
        copy.start()
        ends.append(copy)
    serve(5)
    other_half = pl.ds(pl.multiple_of((1 - c) * share, share), share)
    for d in range(1, nx):
        there = wo.at[xat(-d), other_half]
        remote(there, there, wop_s.at[d - 1], wop_r.at[d - 1], sp=partner).wait_recv()
    for d in order:
        zs = zat(-d)
        remote(mo.at[z], m2.at[zs], m2_s.at[d - 1], m2_r.at[d - 1], sp=zat(d) * 2 + c).wait_recv()
    serve(6)

    top, bottom = [], []
    keep = low(half)
    for p in range(nz // 2):
        a, b = m2[2 * p].astype(F32), m2[2 * p + 1].astype(F32)
        top.append(jnp.where(keep, a, swap(b)).astype(BF16))
        bottom.append(jnp.where(keep, swap(a), b).astype(BF16))
    mixed = jnp.concatenate(
        [jnp.concatenate(top, axis=1), jnp.concatenate(bottom, axis=1)], axis=0
    )
    loads[6].wait()
    chunk = min(512, width)
    square = jnp.zeros((piece, 1), F32)
    for n in range(width // chunk):
        cols = slice(n * chunk, (n + 1) * chunk)
        weight = wo[:, :, cols].reshape(nx * wo.shape[1], chunk)
        added = resid_ref[:, cols].astype(F32) + jnp.dot(
            mixed, weight, preferred_element_type=F32
        )
        added = added.astype(BF16)
        state[:, cols] = added
        added = added.astype(F32)
        square += jnp.sum(added * added, axis=1, keepdims=True)
    factor = lax.rsqrt(square / width + EPS)
    mine_rows = pl.ds(pl.multiple_of(HALO + x * piece, HALO), piece)
    ext[mine_rows] = (state[...].astype(F32) * factor * gain_ref[...]).astype(BF16)

    for d in range(1, nx):
        rows = ext.at[mine_rows]
        copy = remote(rows, rows, nx_s.at[d - 1], nx_r.at[d - 1], tp=xat(d))
        copy.start()
        ends.append(copy)

    rim = ext.at[nx * piece : nx * piece + HALO]
    rims = [
        remote(rim, ext.at[0:HALO], ha_s.at[xp], ha_r, sp=after, tp=xp) for xp in range(nx)
    ]

    @pl.when(last_x)
    def _():
        for copy in rims:
            copy.start()

    serve(7)
    serve(8)
    serve(9)
    for d in range(1, nx):
        rows = ext.at[pl.ds(pl.multiple_of(HALO + xat(-d) * piece, HALO), piece)]
        remote(rows, rows, nx_s.at[d - 1], nx_r.at[d - 1], tp=xat(d)).wait_recv()
    rims[0].wait_recv()

    @pl.when(sp == 0)
    def _():
        ext[0:HALO] = jnp.zeros((HALO, width), BF16)

    def all_across(kind):
        for index in range(nz):
            across(zat(-index), kind, index, 1 - c).wait_recv()

    all_across(0)
    all_across(2)

    chunk = min(256, ff)

    def conv(pre, taps, cols):
        pre = pre.astype(BF16).astype(F32)
        count = taps.shape[0]
        total = taps[0:1, cols] * pre[HALO - count + 1 : HALO - count + 1 + tok]
        for i in range(1, count):
            at = HALO - count + 1 + i
            total = total + taps[i : i + 1, cols] * pre[at : at + tok]
        return total

    for n in range(ff // chunk):
        cols = slice(n * chunk, (n + 1) * chunk)
        gate = jnp.dot(ext[...], wf[:, cols], preferred_element_type=F32)
        value = jnp.dot(
            ext[...], wf[:, ff + n * chunk : ff + (n + 1) * chunk], preferred_element_type=F32
        )
        gate = conv(gate, cg_ref, cols)
        value = conv(value, cv_ref, cols)
        gated[:, cols] = (gate / (1.0 + jnp.exp(-gate)) * value).astype(BF16)

    def rs_copy(d, cols):
        return remote(
            rsb.at[pl.ds(pl.multiple_of(xat(d) * piece, piece), piece), cols],
            rsr.at[d - 1, :, cols], rs_s.at[d - 1], rs_r.at[d - 1], tp=xat(d),
        )

    all_across(1)
    far_first = sorted(range(1, nx), key=lambda d: -min(d, nx - d))
    for n in range(nz // 2):
        sides = []
        for zz in (2 * n, 2 * n + 1):
            sides.append(
                jnp.concatenate(
                    [
                        wf[
                            (zz * 2 + cc) * slab : (zz * 2 + cc + 1) * slab,
                            2 * ff + j * LANES : 2 * ff + (j + 1) * LANES,
                        ]
                        for cc in range(2)
                        for j in range(blocks)
                    ],
                    axis=0,
                )
            )
        part = jnp.dot(
            gated[...], jnp.concatenate(sides, axis=1), preferred_element_type=F32
        )
        cols = slice(n * 2 * LANES, (n + 1) * 2 * LANES)
        pf[:, cols] = part
        rsb[:, cols] = part.astype(BF16)
        for d in far_first:
            rs_copy(d, cols).start()
    everything = slice(0, width)
    total = state[...].astype(F32) + pf[pl.ds(pl.multiple_of(x * piece, piece), piece)]
    for d in range(1, nx):
        rs_copy(d, everything).wait_recv()
        total = total + rsr[d - 1].astype(F32)
    out_ref[...] = total.astype(BF16)

    for copy in ends:
        copy.wait_send()
    for d in range(1, nz):
        remote(mo.at[zat(d)], m2.at[z], m2_s.at[d - 1], m2_r.at[d - 1], sp=zat(d) * 2 + c).wait_send()
    for e in range(1, nx):
        remote(
            s2.at[:, 0:piece], kv.at[:, c, x], s3_s.at[e - 1], s3_r.at[e - 1], tp=xat(e)
        ).wait_send()
        rs_copy(e, everything).wait_send()
        remote(
            wo_ref.at[own_half], wo.at[x, own_half], wo_s.at[e - 1], wo_r.at[e - 1], tp=xat(e)
        ).wait_send()

    @pl.when(last_x)
    def _():
        for copy in rims:
            copy.wait_send()


def body(*args):
    queries, keys, values, resid, out_weight, gate_weight = args[:6]
    nx, nz = lax.axis_size("tp"), lax.axis_size("sp") // 2
    tok, mix = queries.shape
    piece, width = resid.shape
    ff = gate_weight.shape[1]
    slab = gate_weight.shape[0]
    heads = mix // HEAD
    assert heads * nx == nz
    blocks = ff // 2 // slab
    dims = (nx, nz, heads, tok, piece, width, ff, slab)
    packed = piece + piece // 2
    vmem = pltpu.VMEM
    dma = pltpu.SemaphoreType.DMA
    scratch = [
        vmem((tok, mix), BF16),
        vmem((tok, mix), BF16),
        vmem((tok, mix), BF16),
        vmem((piece, width), BF16),
        vmem((HEAD, ff // 2), BF16),
        vmem((nz * piece, LANES), jnp.int32),
        vmem((nx, heads, packed, LANES), BF16),
        vmem((nx, heads, packed, LANES), BF16),
        vmem((nz, packed, LANES), BF16),
        vmem((nz, 2, nx, piece, LANES), BF16),
        vmem((nz * piece, LANES), BF16),
        vmem((tok, tok), BF16),
        vmem((nz * piece, LANES), F32),
        vmem((nz * piece, LANES), F32),
        vmem((nz, piece // 2, LANES), BF16),
        vmem((nz, piece // 2, LANES), BF16),
        vmem((nx, out_weight.shape[0], width), BF16),
        vmem((2 * nz * slab, 2 * ff + blocks * LANES), BF16),
        vmem((HEAD, ff // 2), BF16),
        vmem((piece, width), BF16),
        vmem((HALO + tok, width), BF16),
        vmem((tok, ff), BF16),
        vmem((tok, width), BF16),
        vmem((tok, width), F32),
        vmem((nx - 1, piece, width), BF16),
    ]
    sems = [
        dma((nx - 1,)), dma((nx - 1,)),
        dma((nz - 1,)), dma((nz - 1,)),
        dma((nx - 1,)), dma((nx - 1,)),
        dma((nx,)), dma((nx,)),
        dma((7,)),
        dma((2, nz // 2)), dma((2, nz // 2)),
        dma((2, nz // 2)), dma((2, nz // 2)),
        dma((3, nz)), dma((3, nz)),
        dma((nz,)), dma((nz,)),
        dma, dma((nx - 1,)), dma((nx - 1,)),
        dma((nx - 1,)), dma((nx - 1,)),
        dma((nz - 1,)), dma((nz - 1,)),
        dma((nx - 1,)), dma((nx - 1,)),
        dma((nx,)), dma,
        dma((nx - 1,)), dma((nx - 1,)),
        dma, dma,
    ]
    in_vmem = pl.BlockSpec(memory_space=pltpu.VMEM)
    anywhere = pl.BlockSpec(memory_space=pl.ANY)
    specs = [anywhere] * 7 + [in_vmem] * 3 + [anywhere]
    args = list(args)
    args[9] = args[9].reshape(1, width)
    args[10] = args[10].T
    return pl.pallas_call(
        functools.partial(kernel, dims),
        out_shape=jax.ShapeDtypeStruct((piece, width), BF16),
        in_specs=specs,
        out_specs=in_vmem,
        scratch_shapes=scratch + sems,
        compiler_params=pltpu.CompilerParams(
            collective_id=0, has_side_effects=True, vmem_limit_bytes=66 * 1000 * 1000
        ),
        name="layer",
    )(*args)


def solution(mesh):
    placed = (
        P(("grp", "sp"), "tp"),
        P(("grp", "sp"), "tp"),
        P(("grp", "sp"), "tp"),
        P(("grp", "sp", "tp"), None),
        P("tp", None),
        P("sp", "tp"),
        P("sp", "tp"),
        P(None, "tp"),
        P(None, "tp"),
        P(),
        P("tp", "sp"),
    )
    return jax.shard_map(
        body, mesh=mesh, in_specs=placed, out_specs=P(("grp", "sp", "tp"), None), check_vma=False
    )
```

```python
import functools
import math

import jax
import jax.numpy as jnp
from jax import lax
from jax.experimental import pallas as pl
from jax.experimental.pallas import tpu as pltpu
from jax.sharding import PartitionSpec as P

HEAD = 64
LANES = 128
EPS = 1e-06
GROUPS = 4
HALO = 16
MESH = pl.DeviceIdType.MESH
F32 = jnp.float32
BF16 = jnp.bfloat16
LOG2E = math.log2(math.e)


def kernel(
    dims,
    q_hbm, k_hbm, v_hbm, resid_hbm, wo_ref, gw_ref, vw_ref, cg_ref, cv_ref, gain_ref, dw_ref,
    out_ref,
    q_ref, k_ref, v_ref, resid_ref, dwn, place, pack, s1, s2, kv, qx, tri, acc, later, mo, m2, wo, wf, dpart, state, ext, gated, rsb, pf, rsr,
    s1_s, s1_r, s2_s, s2_r, s3_s, s3_r, sp_s, sp_r, in_l, cw_s, cw_r, cc_s, cc_r, wp_s, wp_r, wy_s, wy_r,
    wo_l, wo_s, wo_r, wop_s, wop_r, m2_s, m2_r, nx_s, nx_r, ha_s, ha_r, rs_s, rs_r, dp_s, dp_r,
):
    nx, nz, heads, tok, piece, width, ff, slab = dims
    half = piece // 2
    down_rows = ff // 2
    blocks = down_rows // slab
    strips = nz // GROUPS
    rows_group = strips * piece
    sp = lax.axis_index("sp")
    x = lax.axis_index("tp")
    z = lax.div(sp, 2)
    c = lax.rem(sp, 2)
    partner = z * 2 + 1 - c
    group = lax.axis_index("grp")
    side = lax.rem(group, 2)
    twin = group + 1 - 2 * side
    low = lambda rows: lax.broadcasted_iota(jnp.int32, (rows, LANES), 1) < HEAD
    swap = lambda a: pltpu.roll(a, HEAD, 1)

    def xat(d):
        return lax.rem(x + d + nx, nx)

    def zat(d):
        return lax.rem(z + d + nz, nz)

    def remote(src, dst, send, recv, **where):
        return pltpu.make_async_remote_copy(
            src_ref=src, dst_ref=dst, send_sem=send, recv_sem=recv, device_id=where,
            device_id_type=MESH,
        )

    def slab_rows(zz, cc):
        return pl.ds(pl.multiple_of((zz * 2 + cc) * slab, slab), slab)

    loads = []
    for i, (src, dst) in enumerate(
        (
            (q_hbm, q_ref),
            (k_hbm, k_ref),
            (v_hbm, v_ref),
            (dw_ref.at[:, pl.ds(pl.multiple_of(c * down_rows, LANES), down_rows)], dwn),
            (gw_ref, wf.at[slab_rows(z, c), 0:ff]),
            (vw_ref, wf.at[slab_rows(z, c), ff : 2 * ff]),
            (resid_hbm, resid_ref),
        )
    ):
        loads.append(pltpu.make_async_copy(src, dst, in_l.at[i]))
        loads[-1].start()
    own_wo = pltpu.make_async_copy(wo_ref, wo.at[x], wo_l)
    own_wo.start()
    for load in loads[:3]:
        load.wait()

    for xp in range(nx):
        at = xp * piece
        for p in range(heads // 2):
            cols = slice(p * LANES, (p + 1) * LANES)
            kk = k_ref[at : at + piece, cols].astype(F32)
            vv = v_ref[at : at + piece, cols].astype(F32)
            qq = q_ref[at : at + piece, cols].astype(F32)
            qr = swap(qq)
            keep = low(piece)
            pack[xp, 2 * p, 0:piece] = jnp.where(keep, kk, swap(vv)).astype(BF16)
            pack[xp, 2 * p + 1, 0:piece] = jnp.where(keep, swap(kk), vv).astype(BF16)
            keep = low(half)
            pack[xp, 2 * p, piece:] = jnp.where(keep, qq[:half], qr[half:]).astype(BF16)
            pack[xp, 2 * p + 1, piece:] = jnp.where(keep, qr[:half], qq[half:]).astype(BF16)
    s1[x] = pack[x]

    barrier = pltpu.get_barrier_semaphore()
    last_x = x == nx - 1
    before = lax.rem(sp + 2 * nz - 1, 2 * nz)
    after = lax.rem(sp + 1, 2 * nz)

    def greet(**where):
        pl.semaphore_signal(barrier, inc=1, device_id=where, device_id_type=MESH)

    for d in range(1, nx):
        greet(tp=xat(d))
    for d in range(1, nz):
        greet(sp=zat(d) * 2 + c)
    greet(sp=partner)
    greet(grp=twin)
    greet(sp=before, tp=nx - 1)

    @pl.when(last_x)
    def _():
        for xp in range(nx):
            greet(sp=after, tp=xp)

    pl.semaphore_wait(barrier, nx - 1 + nz - 1 + 3 + jnp.where(last_x, nx, 0))

    ends = []
    for d in range(1, nx):
        copy = remote(pack.at[xat(d)], s1.at[x], s1_s.at[d - 1], s1_r.at[d - 1], tp=xat(d))
        copy.start()
        ends.append(copy)
    down_part = remote(
        dw_ref.at[:, pl.ds(pl.multiple_of((1 - c) * down_rows, LANES), down_rows)], dpart, dp_s,
        dp_r, sp=partner,
    )
    down_part.start()
    ends.append(down_part)
    share = wo_ref.shape[0] // 2
    own_half = pl.ds(pl.multiple_of(c * share, share), share)
    wo_parts = nz
    wo_cols = width // wo_parts

    def send_wo(part):
        cols = slice(part * wo_cols, (part + 1) * wo_cols)
        for d in range(1, nx):
            remote(
                wo_ref.at[own_half, cols], wo.at[x, own_half, cols], wo_s.at[d - 1],
                wo_r.at[d - 1], tp=xat(d),
            ).start()

    down_part.wait_recv()
    for load in loads[3:6]:
        load.wait()
    mine = dwn[...].astype(F32)
    other = dpart[...].astype(F32)
    first = c == 0
    row = lax.broadcasted_iota(jnp.int32, (HEAD, LANES), 0)
    col = lax.broadcasted_iota(jnp.int32, (HEAD, LANES), 1)
    turn = (((0,), (0,)), ((), ()))
    both = lax.dot_general(
        jnp.where(first, mine, other).astype(BF16), (row == col).astype(BF16), turn,
        preferred_element_type=F32,
    ) + lax.dot_general(
        jnp.where(first, other, mine).astype(BF16), (row + HEAD == col).astype(BF16), turn,
        preferred_element_type=F32,
    )
    both = both.astype(BF16)
    for j in range(blocks):
        wf[slab_rows(z, c), 2 * ff + j * LANES : 2 * ff + (j + 1) * LANES] = both[
            j * slab : (j + 1) * slab
        ]
    hops = (nz // 2, nz - 1 - nz // 2)
    lanes = (
        pl.ds(pl.multiple_of(side * ff, LANES), ff),
        pl.ds(2 * ff, blocks * LANES),
        pl.ds(pl.multiple_of((1 - side) * ff, LANES), ff),
    )

    def slab_part(origin, kind, core=c):
        return wf.at[slab_rows(origin, core), lanes[kind]]

    def from_hops(way, step):
        return zat(-step) if way == 0 else zat(step)

    def ring(way, kind, step, sem):
        part = slab_part(from_hops(way, step), kind)
        sends, recvs = ((cw_s, cw_r), (cc_s, cc_r))[way]
        to = zat(1) if way == 0 else zat(-1)
        return remote(part, part, sends.at[kind, sem], recvs.at[kind, sem], sp=to * 2 + c)

    def across(origin, kind, index, core=c):
        part = slab_part(origin, kind, core)
        return remote(part, part, wp_s.at[kind, index], wp_r.at[kind, index], sp=partner)

    def twin_copy(origin, index, kind=0):
        part = slab_part(origin, kind)
        return remote(part, part, wy_s.at[index], wy_r.at[index], grp=twin)

    def begin(copy):
        copy.start()
        ends.append(copy)

    for kind in range(2):
        for way in range(2):
            begin(ring(way, kind, 0, 0))
    for kind in range(3):
        begin(across(z, kind, 0))

    def serve(step):
        for way in range(2):
            if step <= hops[way]:
                origin, index = from_hops(way, step), step if way == 0 else nz - step
                ring(way, 0, step, step - 1).wait_recv()
                if step < hops[way]:
                    begin(ring(way, 0, step, step))
                begin(twin_copy(origin, index))
                begin(across(origin, 0, index))
        at = step - 1
        for way in range(2):
            if 1 <= at <= hops[way]:
                origin, index = from_hops(way, at), at if way == 0 else nz - at
                ring(way, 1, at, at - 1).wait_recv()
                if at < hops[way]:
                    begin(ring(way, 1, at, at))
                begin(across(origin, 1, index))
                twin_copy(origin, index, 2).wait_recv()
                begin(across(origin, 2, index))

    order = sorted(range(1, nz), key=lambda d: (-min(d, nz - d), d))
    for e in range(1, nx):
        remote(
            pack.at[x], s1.at[xat(-e)], s1_s.at[e - 1], s1_r.at[e - 1], tp=xat(e)
        ).wait_recv()
    s2[z] = s1[lax.div(z, heads), lax.rem(z, heads)]
    for d in order:
        h = zat(d)
        begin(
            remote(
                s1.at[lax.div(h, heads), lax.rem(h, heads)], s2.at[z], s2_s.at[d - 1],
                s2_r.at[d - 1], sp=h * 2 + c,
            )
        )

    r = lax.broadcasted_iota(jnp.int32, (tok, tok), 0)
    s = lax.broadcasted_iota(jnp.int32, (tok, tok), 1)
    tri[...] = (r > s).astype(BF16)
    row = lax.broadcasted_iota(jnp.int32, (nz * piece, LANES), 0)
    strip = lax.div(row, piece)
    place[...] = strip * (2 * tok - piece) + row + c * tok + x * piece
    scale = LOG2E / math.sqrt(HEAD)
    acc[...] = jnp.zeros_like(acc)
    later[...] = jnp.zeros_like(later)
    for d in [0] + order:
        zs = zat(-d)
        if d:
            remote(
                s2.at[z], s2.at[zs], s2_s.at[d - 1], s2_r.at[d - 1], sp=zat(d) * 2 + c
            ).wait_recv()
        kv[zs, c, x] = s2[zs, 0:piece]
        for e in range(1, nx):
            remote(
                s2.at[zs, 0:piece], kv.at[zs, c, x], s3_s.at[e - 1], s3_r.at[e - 1], tp=xat(e)
            ).start()
        packed = s2[zs, piece:].astype(F32)
        keep = low(half)
        at = pl.multiple_of(zs * piece, piece)
        qx[pl.ds(at, half)] = jnp.where(keep, packed, 0.0).astype(BF16)
        qx[pl.ds(pl.multiple_of(at + half, half), half)] = jnp.where(
            keep, swap(packed), 0.0
        ).astype(BF16)
    begin(
        remote(s2.at[:, 0:piece], kv.at[:, c, x], sp_s.at[0], sp_r.at[0], sp=partner)
    )
    for part in range(wo_parts):
        send_wo(part)
    serve(1)
    for e in (1, nx - 1) + tuple(range(2, nx - 1)) if nx > 2 else (1,):
        source = xat(-e)
        got = kv.at[:, c, source]
        remote(
            s2.at[:, 0:piece], got, s3_s.at[e - 1], s3_r.at[e - 1], tp=xat(e)
        ).wait_recv()
        begin(remote(got, got, sp_s.at[e], sp_r.at[e], sp=partner))
    serve(2)
    for e in range(nx):
        there = kv.at[:, 1 - c, xat(-e)]
        remote(there, there, sp_s.at[e], sp_r.at[e], sp=partner).wait_recv()

    tiles = 2 * strips

    def chances(j, rows, masked):
        tile = kv[lax.div(j, 2), lax.rem(j, 2)].reshape(tok, LANES)
        score = lax.dot_general(
            qx[rows], tile, (((1,), (1,)), ((), ())), preferred_element_type=F32
        ) * scale
        neg = jnp.minimum(score, 0.0)
        pos = jnp.maximum(score, 0.0)
        soft = jnp.log2(1.0 + jnp.exp2(neg - pos))
        stay = pos + soft
        seen = None
        if masked:
            where = jnp.concatenate([place[rows]] * (tok // LANES), axis=1)
            seen = lax.broadcasted_iota(jnp.int32, (rows_group, tok), 1) < where - j * tok
            stay = jnp.where(seen, stay, 0.0)
        return tile, neg - soft, stay.astype(BF16), seen

    def weights(tile, go, stay, seen):
        suffix = jnp.dot(stay, tri[...], preferred_element_type=F32)
        weight = jnp.exp2(go - suffix)
        if seen is not None:
            weight = jnp.where(seen, weight, 0.0)
        return tile, weight.astype(BF16), suffix[:, 0:1] + stay[:, 0:1].astype(F32)

    def gather(rows, tile, weight, total):
        behind = later[rows]
        acc[rows] += jnp.exp2(behind) * jnp.dot(weight, tile, preferred_element_type=F32)
        later[rows] = behind - jnp.broadcast_to(total, behind.shape)

    def stretch(low_group, active, unroll):
        unroll = min(tiles, unroll)

        def step(i, carry):
            tasks = [
                (tiles * (low_group + 1) - 1 - i * unroll - u, g)
                for u in range(unroll)
                for g in active
            ]
            held = {}
            for t in range(len(tasks) + 2):
                if t < len(tasks):
                    j, g = tasks[t]
                    held[t] = chances(j, group_rows(g), g == low_group)
                if 1 <= t <= len(tasks):
                    held[t - 1] = weights(*held[t - 1])
                if t >= 2:
                    gather(group_rows(tasks[t - 2][1]), *held.pop(t - 2))
            return carry

        lax.fori_loop(0, tiles // unroll, step, 0)

    def group_rows(g):
        return slice(g * rows_group, (g + 1) * rows_group)

    def send_rows(g):
        for zs in range(g * strips, (g + 1) * strips):
            rows = acc[zs * piece : (zs + 1) * piece]
            mo[zs] = jnp.where(low(half), swap(rows[:half]), rows[half:]).astype(BF16)
        for zs in range(g * strips, (g + 1) * strips):

            @pl.when(z == zs)
            def _():
                m2[zs] = mo[zs]

            @pl.when(z != zs)
            def _():
                d = lax.rem(zs - z + nz, nz) - 1
                remote(mo.at[zs], m2.at[z], m2_s.at[d], m2_r.at[d], sp=zs * 2 + c).start()

    stretch(3, (3,), 4)
    serve(3)
    stretch(2, (2, 3), 2)
    serve(4)
    stretch(1, (1, 2, 3), 2)
    serve(5)
    stretch(0, (2, 3), 2)
    send_rows(3)
    send_rows(2)
    serve(6)
    stretch(0, (0, 1), 2)
    send_rows(1)
    send_rows(0)

    own_wo.wait()
    for d in range(1, nx):
        got = wo.at[xat(-d), own_half]
        remote(wo_ref.at[own_half], got, wo_s.at[d - 1], wo_r.at[d - 1], tp=xat(d)).wait_recv()
        copy = remote(got, got, wop_s.at[d - 1], wop_r.at[d - 1], sp=partner)
        copy.start()
        ends.append(copy)
    serve(7)
    other_half = pl.ds(pl.multiple_of((1 - c) * share, share), share)
    for d in range(1, nx):
        there = wo.at[xat(-d), other_half]
        remote(there, there, wop_s.at[d - 1], wop_r.at[d - 1], sp=partner).wait_recv()
    for d in order:
        zs = zat(-d)
        remote(mo.at[z], m2.at[zs], m2_s.at[d - 1], m2_r.at[d - 1], sp=zat(d) * 2 + c).wait_recv()
    serve(8)

    top, bottom = [], []
    keep = low(half)
    for p in range(nz // 2):
        a, b = m2[2 * p].astype(F32), m2[2 * p + 1].astype(F32)
        top.append(jnp.where(keep, a, swap(b)).astype(BF16))
        bottom.append(jnp.where(keep, swap(a), b).astype(BF16))
    mixed = jnp.concatenate(
        [jnp.concatenate(top, axis=1), jnp.concatenate(bottom, axis=1)], axis=0
    )
    loads[6].wait()
    chunk = min(512, width)
    square = jnp.zeros((piece, 1), F32)
    for n in range(width // chunk):
        cols = slice(n * chunk, (n + 1) * chunk)
        weight = wo[:, :, cols].reshape(nx * wo.shape[1], chunk)
        added = resid_ref[:, cols].astype(F32) + jnp.dot(
            mixed, weight, preferred_element_type=F32
        )
        added = added.astype(BF16)
        state[:, cols] = added
        added = added.astype(F32)
        square += jnp.sum(added * added, axis=1, keepdims=True)
    factor = lax.rsqrt(square / width + EPS)
    mine_rows = pl.ds(pl.multiple_of(HALO + x * piece, HALO), piece)
    ext[mine_rows] = (state[...].astype(F32) * factor * gain_ref[...]).astype(BF16)

    sides = (xat(1), xat(-1))
    halves = (slice(0, width // 2), slice(width // 2, width))

    def normed_half(origin, h):
        return ext.at[pl.ds(pl.multiple_of(HALO + origin * piece, HALO), piece), halves[h]]

    def normed_copy(way, h, origin):
        part = normed_half(origin, h)
        return remote(part, part, nx_s.at[way, h], nx_r.at[way, h], tp=sides[way])

    def normed_on(way, origin):
        part = normed_half(origin, way)
        return remote(part, part, nx_s.at[way, 2], nx_r.at[way, 2], tp=sides[way])

    for turn_h in range(2):
        for way in range(2):
            begin(normed_copy(way, turn_h if way == 0 else 1 - turn_h, x))

    rim = ext.at[nx * piece : nx * piece + HALO]
    rims = [
        remote(rim, ext.at[0:HALO], ha_s.at[xp], ha_r, sp=after, tp=xp) for xp in range(nx)
    ]

    @pl.when(last_x)
    def _():
        for copy in rims:
            copy.start()

    for way in range(2):
        normed_copy(way, way, sides[1 - way]).wait_recv()
        begin(normed_on(way, sides[1 - way]))
    serve(9)
    for way in range(2):
        normed_copy(way, 1 - way, sides[1 - way]).wait_recv()
    for way in range(2):
        normed_on(way, xat(2)).wait_recv()
    rims[0].wait_recv()

    @pl.when(sp == 0)
    def _():
        ext[0:HALO] = jnp.zeros((HALO, width), BF16)

    def all_across(kind):
        for index in range(nz):
            across(zat(-index), kind, index, 1 - c).wait_recv()

    all_across(0)
    all_across(2)

    chunk = min(256, ff)

    def conv(pre, taps, cols):
        pre = pre.astype(BF16).astype(F32)
        count = taps.shape[0]
        total = taps[0:1, cols] * pre[HALO - count + 1 : HALO - count + 1 + tok]
        for i in range(1, count):
            at = HALO - count + 1 + i
            total = total + taps[i : i + 1, cols] * pre[at : at + tok]
        return total

    for n in range(ff // chunk):
        cols = slice(n * chunk, (n + 1) * chunk)
        gate = jnp.dot(ext[...], wf[:, cols], preferred_element_type=F32)
        value = jnp.dot(
            ext[...], wf[:, ff + n * chunk : ff + (n + 1) * chunk], preferred_element_type=F32
        )
        gate = conv(gate, cg_ref, cols)
        value = conv(value, cv_ref, cols)
        gated[:, cols] = (gate / (1.0 + jnp.exp(-gate)) * value).astype(BF16)

    def block_rows(at):
        return pl.ds(pl.multiple_of(at * piece, piece), piece)

    def sum_copy(way, stage, cols):
        at = xat(2) if stage == 0 else sides[way]
        slot = 2 if stage == 0 else way
        return remote(
            rsb.at[block_rows(at), cols], rsr.at[slot, :, cols], rs_s.at[way, stage],
            rs_r.at[way, stage], tp=sides[way],
        )

    all_across(1)
    quarter = nz // 4
    for n in [h * quarter + i for i in range(quarter) for h in range(2)]:
        pair = []
        for zz in (2 * n, 2 * n + 1):
            pair.append(
                jnp.concatenate(
                    [
                        wf[
                            (zz * 2 + cc) * slab : (zz * 2 + cc + 1) * slab,
                            2 * ff + j * LANES : 2 * ff + (j + 1) * LANES,
                        ]
                        for cc in range(2)
                        for j in range(blocks)
                    ],
                    axis=0,
                )
            )
        part = jnp.dot(
            gated[...], jnp.concatenate(pair, axis=1), preferred_element_type=F32
        )
        cols = slice(n * 2 * LANES, (n + 1) * 2 * LANES)
        pf[:, cols] = part
        rsb[:, cols] = part.astype(BF16)
        sum_copy(n // quarter, 0, cols).start()
    for way in range(2):
        begin(sum_copy(way, 1, halves[1 - way]))
    for way in range(2):
        cols = halves[way]
        sum_copy(way, 0, cols).wait_recv()
        rsb[block_rows(sides[way]), cols] = (
            pf[block_rows(sides[way]), cols] + rsr[2, :, cols].astype(F32)
        ).astype(BF16)
        begin(sum_copy(way, 2, cols))
    for h in range(2):
        cols = halves[h]
        sum_copy(1 - h, 1, cols).wait_recv()
        sum_copy(h, 2, cols).wait_recv()
        total = state[:, cols].astype(F32) + pf[block_rows(x), cols]
        total = total + rsr[0, :, cols].astype(F32) + rsr[1, :, cols].astype(F32)
        out_ref[:, cols] = total.astype(BF16)

    for copy in ends:
        copy.wait_send()
    for way in range(2):
        sum_copy(way, 0, halves[way]).wait_send()
    for d in range(1, nz):
        remote(mo.at[zat(d)], m2.at[z], m2_s.at[d - 1], m2_r.at[d - 1], sp=zat(d) * 2 + c).wait_send()
    for e in range(1, nx):
        remote(
            s2.at[:, 0:piece], kv.at[:, c, x], s3_s.at[e - 1], s3_r.at[e - 1], tp=xat(e)
        ).wait_send()
        remote(
            wo_ref.at[own_half], wo.at[x, own_half], wo_s.at[e - 1], wo_r.at[e - 1], tp=xat(e)
        ).wait_send()

    @pl.when(last_x)
    def _():
        for copy in rims:
            copy.wait_send()


def body(*args):
    queries, keys, values, resid, out_weight, gate_weight = args[:6]
    nx, nz = lax.axis_size("tp"), lax.axis_size("sp") // 2
    tok, mix = queries.shape
    piece, width = resid.shape
    ff = gate_weight.shape[1]
    slab = gate_weight.shape[0]
    heads = mix // HEAD
    assert heads * nx == nz and nx == 4
    blocks = ff // 2 // slab
    dims = (nx, nz, heads, tok, piece, width, ff, slab)
    packed = piece + piece // 2
    vmem = pltpu.VMEM
    dma = pltpu.SemaphoreType.DMA
    scratch = [
        vmem((tok, mix), BF16),
        vmem((tok, mix), BF16),
        vmem((tok, mix), BF16),
        vmem((piece, width), BF16),
        vmem((HEAD, ff // 2), BF16),
        vmem((nz * piece, LANES), jnp.int32),
        vmem((nx, heads, packed, LANES), BF16),
        vmem((nx, heads, packed, LANES), BF16),
        vmem((nz, packed, LANES), BF16),
        vmem((nz, 2, nx, piece, LANES), BF16),
        vmem((nz * piece, LANES), BF16),
        vmem((tok, tok), BF16),
        vmem((nz * piece, LANES), F32),
        vmem((nz * piece, LANES), F32),
        vmem((nz, piece // 2, LANES), BF16),
        vmem((nz, piece // 2, LANES), BF16),
        vmem((nx, out_weight.shape[0], width), BF16),
        vmem((2 * nz * slab, 2 * ff + blocks * LANES), BF16),
        vmem((HEAD, ff // 2), BF16),
        vmem((piece, width), BF16),
        vmem((HALO + tok, width), BF16),
        vmem((tok, ff), BF16),
        vmem((tok, width), BF16),
        vmem((tok, width), F32),
        vmem((nx - 1, piece, width), BF16),
    ]
    sems = [
        dma((nx - 1,)), dma((nx - 1,)),
        dma((nz - 1,)), dma((nz - 1,)),
        dma((nx - 1,)), dma((nx - 1,)),
        dma((nx,)), dma((nx,)),
        dma((7,)),
        dma((2, nz // 2)), dma((2, nz // 2)),
        dma((2, nz // 2)), dma((2, nz // 2)),
        dma((3, nz)), dma((3, nz)),
        dma((nz,)), dma((nz,)),
        dma, dma((nx - 1,)), dma((nx - 1,)),
        dma((nx - 1,)), dma((nx - 1,)),
        dma((nz - 1,)), dma((nz - 1,)),
        dma((2, 3)), dma((2, 3)),
        dma((nx,)), dma,
        dma((2, 3)), dma((2, 3)),
        dma, dma,
    ]
    in_vmem = pl.BlockSpec(memory_space=pltpu.VMEM)
    anywhere = pl.BlockSpec(memory_space=pl.ANY)
    specs = [anywhere] * 7 + [in_vmem] * 3 + [anywhere]
    args = list(args)
    args[9] = args[9].reshape(1, width)
    args[10] = args[10].T
    return pl.pallas_call(
        functools.partial(kernel, dims),
        out_shape=jax.ShapeDtypeStruct((piece, width), BF16),
        in_specs=specs,
        out_specs=in_vmem,
        scratch_shapes=scratch + sems,
        compiler_params=pltpu.CompilerParams(
            collective_id=0, has_side_effects=True, vmem_limit_bytes=66 * 1000 * 1000
        ),
        name="layer",
    )(*args)


def solution(mesh):
    placed = (
        P(("grp", "sp"), "tp"),
        P(("grp", "sp"), "tp"),
        P(("grp", "sp"), "tp"),
        P(("grp", "sp", "tp"), None),
        P("tp", None),
        P("sp", "tp"),
        P("sp", "tp"),
        P(None, "tp"),
        P(None, "tp"),
        P(),
        P("tp", "sp"),
    )
    return jax.shard_map(
        body, mesh=mesh, in_specs=placed, out_specs=P(("grp", "sp", "tp"), None), check_vma=False
    )
```

```python
import functools
import math

import jax
import jax.numpy as jnp
from jax import lax
from jax.experimental import pallas as pl
from jax.experimental.pallas import tpu as pltpu
from jax.sharding import PartitionSpec as P

HEAD = 64
LANES = 128
EPS = 1e-06
GROUPS = 4
HALO = 16
MESH = pl.DeviceIdType.MESH
F32 = jnp.float32
BF16 = jnp.bfloat16
LOG2E = math.log2(math.e)


def kernel(
    dims,
    q_hbm, k_hbm, v_hbm, resid_hbm, wo_ref, gw_ref, vw_ref, cg_ref, cv_ref, gain_ref, dw_ref,
    out_ref,
    q_ref, k_ref, v_ref, resid_ref, dwn, place, pack, s1, s2, kv, qx, tri, acc, later, mo, m2, wo, wf, dpart, state, ext, gated, rsb, pf, rsr,
    s1_s, s1_r, s2_s, s2_r, s3_s, s3_r, sp_s, sp_r, in_l, cw_s, cw_r, cc_s, cc_r, wp_s, wp_r, wy_s, wy_r,
    wo_l, wo_s, wo_r, wop_s, wop_r, m2_s, m2_r, nx_s, nx_r, ha_s, ha_r, rs_s, rs_r, dp_s, dp_r,
):
    nx, nz, heads, tok, piece, width, ff, slab = dims
    half = piece // 2
    down_rows = ff // 2
    blocks = down_rows // slab
    strips = nz // GROUPS
    rows_group = strips * piece
    sp = lax.axis_index("sp")
    x = lax.axis_index("tp")
    z = lax.div(sp, 2)
    c = lax.rem(sp, 2)
    partner = z * 2 + 1 - c
    group = lax.axis_index("grp")
    side = lax.rem(group, 2)
    twin = group + 1 - 2 * side
    low = lambda rows: lax.broadcasted_iota(jnp.int32, (rows, LANES), 1) < HEAD
    swap = lambda a: pltpu.roll(a, HEAD, 1)

    def xat(d):
        return lax.rem(x + d + nx, nx)

    def zat(d):
        return lax.rem(z + d + nz, nz)

    def remote(src, dst, send, recv, **where):
        return pltpu.make_async_remote_copy(
            src_ref=src, dst_ref=dst, send_sem=send, recv_sem=recv, device_id=where,
            device_id_type=MESH,
        )

    def slab_rows(zz, cc):
        return pl.ds(pl.multiple_of((zz * 2 + cc) * slab, slab), slab)

    loads = []
    for i, (src, dst) in enumerate(
        (
            (q_hbm, q_ref),
            (k_hbm, k_ref),
            (v_hbm, v_ref),
            (dw_ref.at[:, pl.ds(pl.multiple_of(c * down_rows, LANES), down_rows)], dwn),
            (gw_ref, wf.at[slab_rows(z, c), 0:ff]),
            (vw_ref, wf.at[slab_rows(z, c), ff : 2 * ff]),
            (resid_hbm, resid_ref),
        )
    ):
        loads.append(pltpu.make_async_copy(src, dst, in_l.at[i]))
        loads[-1].start()
    own_wo = pltpu.make_async_copy(wo_ref, wo.at[x], wo_l)
    own_wo.start()
    for load in loads[:3]:
        load.wait()

    for xp in range(nx):
        at = xp * piece
        for p in range(heads // 2):
            cols = slice(p * LANES, (p + 1) * LANES)
            kk = k_ref[at : at + piece, cols].astype(F32)
            vv = v_ref[at : at + piece, cols].astype(F32)
            qq = q_ref[at : at + piece, cols].astype(F32)
            qr = swap(qq)
            keep = low(piece)
            pack[xp, 2 * p, 0:piece] = jnp.where(keep, kk, swap(vv)).astype(BF16)
            pack[xp, 2 * p + 1, 0:piece] = jnp.where(keep, swap(kk), vv).astype(BF16)
            keep = low(half)
            pack[xp, 2 * p, piece:] = jnp.where(keep, qq[:half], qr[half:]).astype(BF16)
            pack[xp, 2 * p + 1, piece:] = jnp.where(keep, qr[:half], qq[half:]).astype(BF16)
    s1[x] = pack[x]

    barrier = pltpu.get_barrier_semaphore()
    last_x = x == nx - 1
    before = lax.rem(sp + 2 * nz - 1, 2 * nz)
    after = lax.rem(sp + 1, 2 * nz)

    def greet(**where):
        pl.semaphore_signal(barrier, inc=1, device_id=where, device_id_type=MESH)

    for d in range(1, nx):
        greet(tp=xat(d))
    for d in range(1, nz):
        greet(sp=zat(d) * 2 + c)
    greet(sp=partner)
    greet(grp=twin)
    greet(sp=before, tp=nx - 1)

    @pl.when(last_x)
    def _():
        for xp in range(nx):
            greet(sp=after, tp=xp)

    pl.semaphore_wait(barrier, nx - 1 + nz - 1 + 3 + jnp.where(last_x, nx, 0))

    ends = []
    for d in range(1, nx):
        copy = remote(pack.at[xat(d)], s1.at[x], s1_s.at[d - 1], s1_r.at[d - 1], tp=xat(d))
        copy.start()
        ends.append(copy)
    down_part = remote(
        dw_ref.at[:, pl.ds(pl.multiple_of((1 - c) * down_rows, LANES), down_rows)], dpart, dp_s,
        dp_r, sp=partner,
    )
    down_part.start()
    ends.append(down_part)
    share = wo_ref.shape[0] // 2
    own_half = pl.ds(pl.multiple_of(c * share, share), share)
    wo_parts = nz
    wo_cols = width // wo_parts

    def send_wo(part):
        cols = slice(part * wo_cols, (part + 1) * wo_cols)
        for d in range(1, nx):
            remote(
                wo_ref.at[own_half, cols], wo.at[x, own_half, cols], wo_s.at[d - 1],
                wo_r.at[d - 1], tp=xat(d),
            ).start()

    down_part.wait_recv()
    for load in loads[3:6]:
        load.wait()
    mine = dwn[...].astype(F32)
    other = dpart[...].astype(F32)
    first = c == 0
    row = lax.broadcasted_iota(jnp.int32, (HEAD, LANES), 0)
    col = lax.broadcasted_iota(jnp.int32, (HEAD, LANES), 1)
    turn = (((0,), (0,)), ((), ()))
    both = lax.dot_general(
        jnp.where(first, mine, other).astype(BF16), (row == col).astype(BF16), turn,
        preferred_element_type=F32,
    ) + lax.dot_general(
        jnp.where(first, other, mine).astype(BF16), (row + HEAD == col).astype(BF16), turn,
        preferred_element_type=F32,
    )
    both = both.astype(BF16)
    for j in range(blocks):
        wf[slab_rows(z, c), 2 * ff + j * LANES : 2 * ff + (j + 1) * LANES] = both[
            j * slab : (j + 1) * slab
        ]
    hops = (nz // 2, nz - 1 - nz // 2)
    lanes = (
        pl.ds(pl.multiple_of(side * ff, LANES), ff),
        pl.ds(2 * ff, blocks * LANES),
        pl.ds(pl.multiple_of((1 - side) * ff, LANES), ff),
    )

    def slab_part(origin, kind, core=c):
        return wf.at[slab_rows(origin, core), lanes[kind]]

    def from_hops(way, step):
        return zat(-step) if way == 0 else zat(step)

    def ring(way, kind, step, sem):
        part = slab_part(from_hops(way, step), kind)
        sends, recvs = ((cw_s, cw_r), (cc_s, cc_r))[way]
        to = zat(1) if way == 0 else zat(-1)
        return remote(part, part, sends.at[kind, sem], recvs.at[kind, sem], sp=to * 2 + c)

    def across(origin, kind, index, core=c):
        part = slab_part(origin, kind, core)
        return remote(part, part, wp_s.at[kind, index], wp_r.at[kind, index], sp=partner)

    def twin_copy(origin, index, kind=0):
        part = slab_part(origin, kind)
        return remote(part, part, wy_s.at[index], wy_r.at[index], grp=twin)

    def begin(copy):
        copy.start()
        ends.append(copy)

    for kind in range(2):
        for way in range(2):
            begin(ring(way, kind, 0, 0))
    for kind in range(3):
        begin(across(z, kind, 0))

    def serve(step):
        for way in range(2):
            if step <= hops[way]:
                origin, index = from_hops(way, step), step if way == 0 else nz - step
                ring(way, 0, step, step - 1).wait_recv()
                if step < hops[way]:
                    begin(ring(way, 0, step, step))
                begin(twin_copy(origin, index))
                begin(across(origin, 0, index))
        at = step - 1
        for way in range(2):
            if 1 <= at <= hops[way]:
                origin, index = from_hops(way, at), at if way == 0 else nz - at
                ring(way, 1, at, at - 1).wait_recv()
                if at < hops[way]:
                    begin(ring(way, 1, at, at))
                begin(across(origin, 1, index))
                twin_copy(origin, index, 2).wait_recv()
                begin(across(origin, 2, index))

    order = sorted(range(1, nz), key=lambda d: (min(d, nz - d), d))
    for e in range(1, nx):
        remote(
            pack.at[x], s1.at[xat(-e)], s1_s.at[e - 1], s1_r.at[e - 1], tp=xat(e)
        ).wait_recv()
    s2[z] = s1[lax.div(z, heads), lax.rem(z, heads)]
    spans = (slice(0, piece), slice(piece, piece + half))
    for kind in range(2):
        for d in order:
            h = zat(d)
            begin(
                remote(
                    s1.at[lax.div(h, heads), lax.rem(h, heads), spans[kind]],
                    s2.at[z, spans[kind]], s2_s.at[kind, d - 1], s2_r.at[kind, d - 1],
                    sp=h * 2 + c,
                )
            )

    def arrived(kind, d):
        part = s2.at[zat(-d), spans[kind]]
        remote(
            part, part, s2_s.at[kind, d - 1], s2_r.at[kind, d - 1], sp=zat(d) * 2 + c
        ).wait_recv()

    r = lax.broadcasted_iota(jnp.int32, (tok, tok), 0)
    s = lax.broadcasted_iota(jnp.int32, (tok, tok), 1)
    tri[...] = (r > s).astype(BF16)
    row = lax.broadcasted_iota(jnp.int32, (nz * piece, LANES), 0)
    strip = lax.div(row, piece)
    place[...] = strip * (2 * tok - piece) + row + c * tok + x * piece
    scale = LOG2E / math.sqrt(HEAD)
    acc[...] = jnp.zeros_like(acc)
    later[...] = jnp.zeros_like(later)
    for d in [0] + order:
        zs = zat(-d)
        if d:
            arrived(0, d)
        kv[zs, c, x] = s2[zs, 0:piece]
        for e in range(1, nx):
            remote(
                s2.at[zs, 0:piece], kv.at[zs, c, x], s3_s.at[e - 1], s3_r.at[e - 1], tp=xat(e)
            ).start()
    begin(
        remote(s2.at[:, 0:piece], kv.at[:, c, x], sp_s.at[0], sp_r.at[0], sp=partner)
    )
    for part in range(wo_parts):
        send_wo(part)
    serve(1)
    for e in (1, nx - 1) + tuple(range(2, nx - 1)) if nx > 2 else (1,):
        source = xat(-e)
        got = kv.at[:, c, source]
        remote(
            s2.at[:, 0:piece], got, s3_s.at[e - 1], s3_r.at[e - 1], tp=xat(e)
        ).wait_recv()
        begin(remote(got, got, sp_s.at[e], sp_r.at[e], sp=partner))
    serve(2)
    for d in [0] + order:
        zs = zat(-d)
        if d:
            arrived(1, d)
        packed = s2[zs, piece:].astype(F32)
        keep = low(half)
        at = pl.multiple_of(zs * piece, piece)
        qx[pl.ds(at, half)] = jnp.where(keep, packed, 0.0).astype(BF16)
        qx[pl.ds(pl.multiple_of(at + half, half), half)] = jnp.where(
            keep, swap(packed), 0.0
        ).astype(BF16)
    for e in range(nx):
        there = kv.at[:, 1 - c, xat(-e)]
        remote(there, there, sp_s.at[e], sp_r.at[e], sp=partner).wait_recv()

    tiles = 2 * strips

    def chances(j, rows, masked):
        tile = kv[lax.div(j, 2), lax.rem(j, 2)].reshape(tok, LANES)
        score = lax.dot_general(
            qx[rows], tile, (((1,), (1,)), ((), ())), preferred_element_type=F32
        ) * scale
        neg = jnp.minimum(score, 0.0)
        pos = jnp.maximum(score, 0.0)
        soft = jnp.log2(1.0 + jnp.exp2(neg - pos))
        stay = pos + soft
        seen = None
        if masked:
            where = jnp.concatenate([place[rows]] * (tok // LANES), axis=1)
            seen = lax.broadcasted_iota(jnp.int32, (rows_group, tok), 1) < where - j * tok
            stay = jnp.where(seen, stay, 0.0)
        return tile, neg - soft, stay.astype(BF16), seen

    def weights(tile, go, stay, seen):
        suffix = jnp.dot(stay, tri[...], preferred_element_type=F32)
        weight = jnp.exp2(go - suffix)
        if seen is not None:
            weight = jnp.where(seen, weight, 0.0)
        return tile, weight.astype(BF16), suffix[:, 0:1] + stay[:, 0:1].astype(F32)

    def gather(rows, tile, weight, total):
        behind = later[rows]
        acc[rows] += jnp.exp2(behind) * jnp.dot(weight, tile, preferred_element_type=F32)
        later[rows] = behind - jnp.broadcast_to(total, behind.shape)

    def stretch(low_group, active, unroll):
        unroll = min(tiles, unroll)

        def step(i, carry):
            tasks = [
                (tiles * (low_group + 1) - 1 - i * unroll - u, g)
                for u in range(unroll)
                for g in active
            ]
            held = {}
            for t in range(len(tasks) + 2):
                if t < len(tasks):
                    j, g = tasks[t]
                    held[t] = chances(j, group_rows(g), g == low_group)
                if 1 <= t <= len(tasks):
                    held[t - 1] = weights(*held[t - 1])
                if t >= 2:
                    gather(group_rows(tasks[t - 2][1]), *held.pop(t - 2))
            return carry

        lax.fori_loop(0, tiles // unroll, step, 0)

    def group_rows(g):
        return slice(g * rows_group, (g + 1) * rows_group)

    def send_rows(g):
        for zs in range(g * strips, (g + 1) * strips):
            rows = acc[zs * piece : (zs + 1) * piece]
            mo[zs] = jnp.where(low(half), swap(rows[:half]), rows[half:]).astype(BF16)
        for zs in range(g * strips, (g + 1) * strips):

            @pl.when(z == zs)
            def _():
                m2[zs] = mo[zs]

            @pl.when(z != zs)
            def _():
                d = lax.rem(zs - z + nz, nz) - 1
                remote(mo.at[zs], m2.at[z], m2_s.at[d], m2_r.at[d], sp=zs * 2 + c).start()

    stretch(3, (3,), 4)
    stretch(2, (2, 3), 2)
    serve(3)
    stretch(1, (1, 2, 3), 2)
    serve(4)
    stretch(0, (2, 3), 2)
    send_rows(3)
    send_rows(2)
    serve(5)
    stretch(0, (0, 1), 2)
    send_rows(1)
    send_rows(0)

    own_wo.wait()
    for d in range(1, nx):
        got = wo.at[xat(-d), own_half]
        remote(wo_ref.at[own_half], got, wo_s.at[d - 1], wo_r.at[d - 1], tp=xat(d)).wait_recv()
        copy = remote(got, got, wop_s.at[d - 1], wop_r.at[d - 1], sp=partner)
        copy.start()
        ends.append(copy)
    serve(6)
    other_half = pl.ds(pl.multiple_of((1 - c) * share, share), share)
    for d in range(1, nx):
        there = wo.at[xat(-d), other_half]
        remote(there, there, wop_s.at[d - 1], wop_r.at[d - 1], sp=partner).wait_recv()
    for d in order:
        zs = zat(-d)
        remote(mo.at[z], m2.at[zs], m2_s.at[d - 1], m2_r.at[d - 1], sp=zat(d) * 2 + c).wait_recv()
    serve(7)

    top, bottom = [], []
    keep = low(half)
    for p in range(nz // 2):
        a, b = m2[2 * p].astype(F32), m2[2 * p + 1].astype(F32)
        top.append(jnp.where(keep, a, swap(b)).astype(BF16))
        bottom.append(jnp.where(keep, swap(a), b).astype(BF16))
    mixed = jnp.concatenate(
        [jnp.concatenate(top, axis=1), jnp.concatenate(bottom, axis=1)], axis=0
    )
    loads[6].wait()
    chunk = min(512, width)
    square = jnp.zeros((piece, 1), F32)
    for n in range(width // chunk):
        cols = slice(n * chunk, (n + 1) * chunk)
        weight = wo[:, :, cols].reshape(nx * wo.shape[1], chunk)
        added = resid_ref[:, cols].astype(F32) + jnp.dot(
            mixed, weight, preferred_element_type=F32
        )
        added = added.astype(BF16)
        state[:, cols] = added
        added = added.astype(F32)
        square += jnp.sum(added * added, axis=1, keepdims=True)
    factor = lax.rsqrt(square / width + EPS)
    mine_rows = pl.ds(pl.multiple_of(HALO + x * piece, HALO), piece)
    ext[mine_rows] = (state[...].astype(F32) * factor * gain_ref[...]).astype(BF16)

    sides = (xat(1), xat(-1))
    halves = (slice(0, width // 2), slice(width // 2, width))

    def normed_half(origin, h):
        return ext.at[pl.ds(pl.multiple_of(HALO + origin * piece, HALO), piece), halves[h]]

    def normed_copy(way, h, origin):
        part = normed_half(origin, h)
        return remote(part, part, nx_s.at[way, h], nx_r.at[way, h], tp=sides[way])

    def normed_on(way, origin):
        part = normed_half(origin, way)
        return remote(part, part, nx_s.at[way, 2], nx_r.at[way, 2], tp=sides[way])

    for turn_h in range(2):
        for way in range(2):
            begin(normed_copy(way, turn_h if way == 0 else 1 - turn_h, x))

    rim = ext.at[nx * piece : nx * piece + HALO]
    rims = [
        remote(rim, ext.at[0:HALO], ha_s.at[xp], ha_r, sp=after, tp=xp) for xp in range(nx)
    ]

    @pl.when(last_x)
    def _():
        for copy in rims:
            copy.start()

    for way in range(2):
        normed_copy(way, way, sides[1 - way]).wait_recv()
        begin(normed_on(way, sides[1 - way]))
    serve(8)
    serve(9)
    for way in range(2):
        normed_copy(way, 1 - way, sides[1 - way]).wait_recv()
    for way in range(2):
        normed_on(way, xat(2)).wait_recv()
    rims[0].wait_recv()

    @pl.when(sp == 0)
    def _():
        ext[0:HALO] = jnp.zeros((HALO, width), BF16)

    def all_across(kind):
        for index in range(nz):
            across(zat(-index), kind, index, 1 - c).wait_recv()

    all_across(0)
    all_across(2)

    chunk = min(256, ff)

    def conv(pre, taps, cols):
        pre = pre.astype(BF16).astype(F32)
        count = taps.shape[0]
        total = taps[0:1, cols] * pre[HALO - count + 1 : HALO - count + 1 + tok]
        for i in range(1, count):
            at = HALO - count + 1 + i
            total = total + taps[i : i + 1, cols] * pre[at : at + tok]
        return total

    for n in range(ff // chunk):
        cols = slice(n * chunk, (n + 1) * chunk)
        gate = jnp.dot(ext[...], wf[:, cols], preferred_element_type=F32)
        value = jnp.dot(
            ext[...], wf[:, ff + n * chunk : ff + (n + 1) * chunk], preferred_element_type=F32
        )
        gate = conv(gate, cg_ref, cols)
        value = conv(value, cv_ref, cols)
        gated[:, cols] = (gate / (1.0 + jnp.exp(-gate)) * value).astype(BF16)

    def block_rows(at):
        return pl.ds(pl.multiple_of(at * piece, piece), piece)

    def sum_copy(way, stage, cols):
        at = xat(2) if stage == 0 else sides[way]
        slot = 2 if stage == 0 else way
        return remote(
            rsb.at[block_rows(at), cols], rsr.at[slot, :, cols], rs_s.at[way, stage],
            rs_r.at[way, stage], tp=sides[way],
        )

    all_across(1)
    quarter = nz // 4
    for n in [h * quarter + i for i in range(quarter) for h in range(2)]:
        pair = []
        for zz in (2 * n, 2 * n + 1):
            pair.append(
                jnp.concatenate(
                    [
                        wf[
                            (zz * 2 + cc) * slab : (zz * 2 + cc + 1) * slab,
                            2 * ff + j * LANES : 2 * ff + (j + 1) * LANES,
                        ]
                        for cc in range(2)
                        for j in range(blocks)
                    ],
                    axis=0,
                )
            )
        part = jnp.dot(
            gated[...], jnp.concatenate(pair, axis=1), preferred_element_type=F32
        )
        cols = slice(n * 2 * LANES, (n + 1) * 2 * LANES)
        pf[:, cols] = part
        rsb[:, cols] = part.astype(BF16)
        sum_copy(n // quarter, 0, cols).start()
    for way in range(2):
        begin(sum_copy(way, 1, halves[1 - way]))
    for way in range(2):
        cols = halves[way]
        sum_copy(way, 0, cols).wait_recv()
        rsb[block_rows(sides[way]), cols] = (
            pf[block_rows(sides[way]), cols] + rsr[2, :, cols].astype(F32)
        ).astype(BF16)
        begin(sum_copy(way, 2, cols))
    for h in range(2):
        cols = halves[h]
        sum_copy(1 - h, 1, cols).wait_recv()
        sum_copy(h, 2, cols).wait_recv()
        total = state[:, cols].astype(F32) + pf[block_rows(x), cols]
        total = total + rsr[0, :, cols].astype(F32) + rsr[1, :, cols].astype(F32)
        out_ref[:, cols] = total.astype(BF16)

    for copy in ends:
        copy.wait_send()
    for way in range(2):
        sum_copy(way, 0, halves[way]).wait_send()
    for d in range(1, nz):
        remote(mo.at[zat(d)], m2.at[z], m2_s.at[d - 1], m2_r.at[d - 1], sp=zat(d) * 2 + c).wait_send()
    for e in range(1, nx):
        remote(
            s2.at[:, 0:piece], kv.at[:, c, x], s3_s.at[e - 1], s3_r.at[e - 1], tp=xat(e)
        ).wait_send()
        remote(
            wo_ref.at[own_half], wo.at[x, own_half], wo_s.at[e - 1], wo_r.at[e - 1], tp=xat(e)
        ).wait_send()

    @pl.when(last_x)
    def _():
        for copy in rims:
            copy.wait_send()


def body(*args):
    queries, keys, values, resid, out_weight, gate_weight = args[:6]
    nx, nz = lax.axis_size("tp"), lax.axis_size("sp") // 2
    tok, mix = queries.shape
    piece, width = resid.shape
    ff = gate_weight.shape[1]
    slab = gate_weight.shape[0]
    heads = mix // HEAD
    assert heads * nx == nz and nx == 4
    blocks = ff // 2 // slab
    dims = (nx, nz, heads, tok, piece, width, ff, slab)
    packed = piece + piece // 2
    vmem = pltpu.VMEM
    dma = pltpu.SemaphoreType.DMA
    scratch = [
        vmem((tok, mix), BF16),
        vmem((tok, mix), BF16),
        vmem((tok, mix), BF16),
        vmem((piece, width), BF16),
        vmem((HEAD, ff // 2), BF16),
        vmem((nz * piece, LANES), jnp.int32),
        vmem((nx, heads, packed, LANES), BF16),
        vmem((nx, heads, packed, LANES), BF16),
        vmem((nz, packed, LANES), BF16),
        vmem((nz, 2, nx, piece, LANES), BF16),
        vmem((nz * piece, LANES), BF16),
        vmem((tok, tok), BF16),
        vmem((nz * piece, LANES), F32),
        vmem((nz * piece, LANES), F32),
        vmem((nz, piece // 2, LANES), BF16),
        vmem((nz, piece // 2, LANES), BF16),
        vmem((nx, out_weight.shape[0], width), BF16),
        vmem((2 * nz * slab, 2 * ff + blocks * LANES), BF16),
        vmem((HEAD, ff // 2), BF16),
        vmem((piece, width), BF16),
        vmem((HALO + tok, width), BF16),
        vmem((tok, ff), BF16),
        vmem((tok, width), BF16),
        vmem((tok, width), F32),
        vmem((nx - 1, piece, width), BF16),
    ]
    sems = [
        dma((nx - 1,)), dma((nx - 1,)),
        dma((2, nz - 1)), dma((2, nz - 1)),
        dma((nx - 1,)), dma((nx - 1,)),
        dma((nx,)), dma((nx,)),
        dma((7,)),
        dma((2, nz // 2)), dma((2, nz // 2)),
        dma((2, nz // 2)), dma((2, nz // 2)),
        dma((3, nz)), dma((3, nz)),
        dma((nz,)), dma((nz,)),
        dma, dma((nx - 1,)), dma((nx - 1,)),
        dma((nx - 1,)), dma((nx - 1,)),
        dma((nz - 1,)), dma((nz - 1,)),
        dma((2, 3)), dma((2, 3)),
        dma((nx,)), dma,
        dma((2, 3)), dma((2, 3)),
        dma, dma,
    ]
    in_vmem = pl.BlockSpec(memory_space=pltpu.VMEM)
    anywhere = pl.BlockSpec(memory_space=pl.ANY)
    specs = [anywhere] * 7 + [in_vmem] * 3 + [anywhere]
    args = list(args)
    args[9] = args[9].reshape(1, width)
    args[10] = args[10].T
    return pl.pallas_call(
        functools.partial(kernel, dims),
        out_shape=jax.ShapeDtypeStruct((piece, width), BF16),
        in_specs=specs,
        out_specs=in_vmem,
        scratch_shapes=scratch + sems,
        compiler_params=pltpu.CompilerParams(
            collective_id=0, has_side_effects=True, vmem_limit_bytes=66 * 1000 * 1000
        ),
        name="layer",
    )(*args)


def solution(mesh):
    placed = (
        P(("grp", "sp"), "tp"),
        P(("grp", "sp"), "tp"),
        P(("grp", "sp"), "tp"),
        P(("grp", "sp", "tp"), None),
        P("tp", None),
        P("sp", "tp"),
        P("sp", "tp"),
        P(None, "tp"),
        P(None, "tp"),
        P(),
        P("tp", "sp"),
    )
    return jax.shard_map(
        body, mesh=mesh, in_specs=placed, out_specs=P(("grp", "sp", "tp"), None), check_vma=False
    )
```

```python
import functools
import math

import jax
import jax.numpy as jnp
from jax import lax
from jax.experimental import pallas as pl
from jax.experimental.pallas import tpu as pltpu
from jax.sharding import PartitionSpec as P

HEAD = 64
LANES = 128
EPS = 1e-06
GROUPS = 4
HALO = 16
MESH = pl.DeviceIdType.MESH
F32 = jnp.float32
BF16 = jnp.bfloat16
LOG2E = math.log2(math.e)


def kernel(
    dims,
    q_hbm, k_hbm, v_hbm, resid_hbm, wo_ref, gw_ref, vw_ref, cg_ref, cv_ref, gain_ref, dw_ref,
    out_ref,
    q_ref, k_ref, v_ref, resid_ref, dwn, place, pack, s1, s2, kv, qx, tri, acc, later, mo, m2, wo, wf, dpart, state, ext, gated, rsb, pf, rsr,
    s1_s, s1_r, s2_s, s2_r, s3_s, s3_r, sp_s, sp_r, in_l, cw_s, cw_r, cc_s, cc_r, wp_s, wp_r, wy_s, wy_r,
    wo_l, wo_s, wo_r, wop_s, wop_r, m2_s, m2_r, nx_s, nx_r, ha_s, ha_r, rs_s, rs_r, dp_s, dp_r,
):
    nx, nz, heads, tok, piece, width, ff, slab = dims
    half = piece // 2
    down_rows = ff // 2
    blocks = down_rows // slab
    strips = nz // GROUPS
    rows_group = strips * piece
    sp = lax.axis_index("sp")
    x = lax.axis_index("tp")
    z = lax.div(sp, 2)
    c = lax.rem(sp, 2)
    partner = z * 2 + 1 - c
    group = lax.axis_index("grp")
    side = lax.rem(group, 2)
    twin = group + 1 - 2 * side
    low = lambda rows: lax.broadcasted_iota(jnp.int32, (rows, LANES), 1) < HEAD
    swap = lambda a: pltpu.roll(a, HEAD, 1)

    def xat(d):
        return lax.rem(x + d + nx, nx)

    def zat(d):
        return lax.rem(z + d + nz, nz)

    def remote(src, dst, send, recv, **where):
        return pltpu.make_async_remote_copy(
            src_ref=src, dst_ref=dst, send_sem=send, recv_sem=recv, device_id=where,
            device_id_type=MESH,
        )

    def slab_rows(zz, cc):
        return pl.ds(pl.multiple_of((zz * 2 + cc) * slab, slab), slab)

    loads = []
    for i, (src, dst) in enumerate(
        (
            (q_hbm, q_ref),
            (k_hbm, k_ref),
            (v_hbm, v_ref),
            (dw_ref.at[:, pl.ds(pl.multiple_of(c * down_rows, LANES), down_rows)], dwn),
            (gw_ref, wf.at[slab_rows(z, c), 0:ff]),
            (vw_ref, wf.at[slab_rows(z, c), ff : 2 * ff]),
            (resid_hbm, resid_ref),
        )
    ):
        loads.append(pltpu.make_async_copy(src, dst, in_l.at[i]))
        loads[-1].start()
    own_wo = pltpu.make_async_copy(wo_ref, wo.at[x], wo_l)
    own_wo.start()
    for load in loads[:3]:
        load.wait()

    for xp in range(nx):
        at = xp * piece
        for p in range(heads // 2):
            cols = slice(p * LANES, (p + 1) * LANES)
            kk = k_ref[at : at + piece, cols].astype(F32)
            vv = v_ref[at : at + piece, cols].astype(F32)
            qq = q_ref[at : at + piece, cols].astype(F32)
            qr = swap(qq)
            keep = low(piece)
            pack[xp, 2 * p, 0:piece] = jnp.where(keep, kk, swap(vv)).astype(BF16)
            pack[xp, 2 * p + 1, 0:piece] = jnp.where(keep, swap(kk), vv).astype(BF16)
            keep = low(half)
            pack[xp, 2 * p, piece:] = jnp.where(keep, qq[:half], qr[half:]).astype(BF16)
            pack[xp, 2 * p + 1, piece:] = jnp.where(keep, qr[:half], qq[half:]).astype(BF16)
    s1[x] = pack[x]

    barrier = pltpu.get_barrier_semaphore()
    last_x = x == nx - 1
    before = lax.rem(sp + 2 * nz - 1, 2 * nz)
    after = lax.rem(sp + 1, 2 * nz)

    def greet(**where):
        pl.semaphore_signal(barrier, inc=1, device_id=where, device_id_type=MESH)

    for d in range(1, nx):
        greet(tp=xat(d))
    for d in range(1, nz):
        greet(sp=zat(d) * 2 + c)
    greet(sp=partner)
    greet(grp=twin)
    greet(sp=before, tp=nx - 1)

    @pl.when(last_x)
    def _():
        for xp in range(nx):
            greet(sp=after, tp=xp)

    pl.semaphore_wait(barrier, nx - 1 + nz - 1 + 3 + jnp.where(last_x, nx, 0))

    spans = (slice(0, piece), slice(piece, piece + half))
    ends = []

    def begin(copy):
        copy.start()
        ends.append(copy)

    for kind in range(2):
        for d in range(1, nx):
            begin(
                remote(
                    pack.at[xat(d), :, spans[kind]], s1.at[x, :, spans[kind]],
                    s1_s.at[kind, d - 1], s1_r.at[kind, d - 1], tp=xat(d),
                )
            )
    down_part = remote(
        dw_ref.at[:, pl.ds(pl.multiple_of((1 - c) * down_rows, LANES), down_rows)], dpart, dp_s,
        dp_r, sp=partner,
    )
    down_part.start()
    ends.append(down_part)
    share = wo_ref.shape[0] // 2
    own_half = pl.ds(pl.multiple_of(c * share, share), share)
    wo_parts = nz
    wo_cols = width // wo_parts

    def send_wo(part):
        cols = slice(part * wo_cols, (part + 1) * wo_cols)
        for d in range(1, nx):
            remote(
                wo_ref.at[own_half, cols], wo.at[x, own_half, cols], wo_s.at[d - 1],
                wo_r.at[d - 1], tp=xat(d),
            ).start()

    down_part.wait_recv()
    for load in loads[3:6]:
        load.wait()
    mine = dwn[...].astype(F32)
    other = dpart[...].astype(F32)
    first = c == 0
    row = lax.broadcasted_iota(jnp.int32, (HEAD, LANES), 0)
    col = lax.broadcasted_iota(jnp.int32, (HEAD, LANES), 1)
    turn = (((0,), (0,)), ((), ()))
    both = lax.dot_general(
        jnp.where(first, mine, other).astype(BF16), (row == col).astype(BF16), turn,
        preferred_element_type=F32,
    ) + lax.dot_general(
        jnp.where(first, other, mine).astype(BF16), (row + HEAD == col).astype(BF16), turn,
        preferred_element_type=F32,
    )
    both = both.astype(BF16)
    for j in range(blocks):
        wf[slab_rows(z, c), 2 * ff + j * LANES : 2 * ff + (j + 1) * LANES] = both[
            j * slab : (j + 1) * slab
        ]
    hops = (nz // 2, nz - 1 - nz // 2)
    lanes = (
        pl.ds(pl.multiple_of(side * ff, LANES), ff),
        pl.ds(2 * ff, blocks * LANES),
        pl.ds(pl.multiple_of((1 - side) * ff, LANES), ff),
    )

    def slab_part(origin, kind, core=c):
        return wf.at[slab_rows(origin, core), lanes[kind]]

    def from_hops(way, step):
        return zat(-step) if way == 0 else zat(step)

    def ring(way, kind, step, sem):
        part = slab_part(from_hops(way, step), kind)
        sends, recvs = ((cw_s, cw_r), (cc_s, cc_r))[way]
        to = zat(1) if way == 0 else zat(-1)
        return remote(part, part, sends.at[kind, sem], recvs.at[kind, sem], sp=to * 2 + c)

    def across(origin, kind, index, core=c):
        part = slab_part(origin, kind, core)
        return remote(part, part, wp_s.at[kind, index], wp_r.at[kind, index], sp=partner)

    def twin_copy(origin, index, kind=0):
        part = slab_part(origin, kind)
        return remote(part, part, wy_s.at[index], wy_r.at[index], grp=twin)

    for kind in range(2):
        for way in range(2):
            begin(ring(way, kind, 0, 0))
    for kind in range(3):
        begin(across(z, kind, 0))

    def serve(step):
        for way in range(2):
            if step <= hops[way]:
                origin, index = from_hops(way, step), step if way == 0 else nz - step
                ring(way, 0, step, step - 1).wait_recv()
                if step < hops[way]:
                    begin(ring(way, 0, step, step))
                begin(twin_copy(origin, index))
                begin(across(origin, 0, index))
        at = step - 1
        for way in range(2):
            if 1 <= at <= hops[way]:
                origin, index = from_hops(way, at), at if way == 0 else nz - at
                ring(way, 1, at, at - 1).wait_recv()
                if at < hops[way]:
                    begin(ring(way, 1, at, at))
                begin(across(origin, 1, index))
                twin_copy(origin, index, 2).wait_recv()
                begin(across(origin, 2, index))

    order = sorted(range(1, nz), key=lambda d: (min(d, nz - d), d))
    for kind in range(2):
        for e in range(1, nx):
            part = s1.at[xat(-e), :, spans[kind]]
            remote(part, part, s1_s.at[kind, e - 1], s1_r.at[kind, e - 1], tp=xat(e)).wait_recv()
        s2[z, spans[kind]] = s1[lax.div(z, heads), lax.rem(z, heads), spans[kind]]
        for d in order:
            h = zat(d)
            begin(
                remote(
                    s1.at[lax.div(h, heads), lax.rem(h, heads), spans[kind]],
                    s2.at[z, spans[kind]], s2_s.at[kind, d - 1], s2_r.at[kind, d - 1],
                    sp=h * 2 + c,
                )
            )

    def arrived(kind, d):
        part = s2.at[zat(-d), spans[kind]]
        remote(
            part, part, s2_s.at[kind, d - 1], s2_r.at[kind, d - 1], sp=zat(d) * 2 + c
        ).wait_recv()

    r = lax.broadcasted_iota(jnp.int32, (tok, tok), 0)
    s = lax.broadcasted_iota(jnp.int32, (tok, tok), 1)
    tri[...] = (r > s).astype(BF16)
    row = lax.broadcasted_iota(jnp.int32, (nz * piece, LANES), 0)
    strip = lax.div(row, piece)
    place[...] = strip * (2 * tok - piece) + row + c * tok + x * piece
    scale = LOG2E / math.sqrt(HEAD)
    acc[...] = jnp.zeros_like(acc)
    later[...] = jnp.zeros_like(later)
    for d in [0] + order:
        zs = zat(-d)
        if d:
            arrived(0, d)
        kv[zs, c, x] = s2[zs, 0:piece]
        for e in range(1, nx):
            remote(
                s2.at[zs, 0:piece], kv.at[zs, c, x], s3_s.at[e - 1], s3_r.at[e - 1], tp=xat(e)
            ).start()
    begin(
        remote(s2.at[:, 0:piece], kv.at[:, c, x], sp_s.at[0], sp_r.at[0], sp=partner)
    )
    for part in range(wo_parts):
        send_wo(part)
    serve(1)
    for e in (1, nx - 1) + tuple(range(2, nx - 1)) if nx > 2 else (1,):
        source = xat(-e)
        got = kv.at[:, c, source]
        remote(
            s2.at[:, 0:piece], got, s3_s.at[e - 1], s3_r.at[e - 1], tp=xat(e)
        ).wait_recv()
        begin(remote(got, got, sp_s.at[e], sp_r.at[e], sp=partner))
    serve(2)
    for d in [0] + order:
        zs = zat(-d)
        if d:
            arrived(1, d)
        packed = s2[zs, piece:].astype(F32)
        keep = low(half)
        at = pl.multiple_of(zs * piece, piece)
        qx[pl.ds(at, half)] = jnp.where(keep, packed, 0.0).astype(BF16)
        qx[pl.ds(pl.multiple_of(at + half, half), half)] = jnp.where(
            keep, swap(packed), 0.0
        ).astype(BF16)
    for e in range(nx):
        there = kv.at[:, 1 - c, xat(-e)]
        remote(there, there, sp_s.at[e], sp_r.at[e], sp=partner).wait_recv()

    tiles = 2 * strips

    def chances(j, rows, masked):
        tile = kv[lax.div(j, 2), lax.rem(j, 2)].reshape(tok, LANES)
        score = lax.dot_general(
            qx[rows], tile, (((1,), (1,)), ((), ())), preferred_element_type=F32
        ) * scale
        neg = jnp.minimum(score, 0.0)
        pos = jnp.maximum(score, 0.0)
        soft = jnp.log2(1.0 + jnp.exp2(neg - pos))
        stay = pos + soft
        seen = None
        if masked:
            where = jnp.concatenate([place[rows]] * (tok // LANES), axis=1)
            seen = lax.broadcasted_iota(jnp.int32, (rows_group, tok), 1) < where - j * tok
            stay = jnp.where(seen, stay, 0.0)
        return tile, neg - soft, stay.astype(BF16), seen

    def weights(tile, go, stay, seen):
        suffix = jnp.dot(stay, tri[...], preferred_element_type=F32)
        weight = jnp.exp2(go - suffix)
        if seen is not None:
            weight = jnp.where(seen, weight, 0.0)
        return tile, weight.astype(BF16), suffix[:, 0:1] + stay[:, 0:1].astype(F32)

    def gather(rows, tile, weight, total):
        behind = later[rows]
        acc[rows] += jnp.exp2(behind) * jnp.dot(weight, tile, preferred_element_type=F32)
        later[rows] = behind - jnp.broadcast_to(total, behind.shape)

    def stretch(low_group, active, unroll):
        unroll = min(tiles, unroll)

        def step(i, carry):
            tasks = [
                (tiles * (low_group + 1) - 1 - i * unroll - u, g)
                for u in range(unroll)
                for g in active
            ]
            held = {}
            for t in range(len(tasks) + 2):
                if t < len(tasks):
                    j, g = tasks[t]
                    held[t] = chances(j, group_rows(g), g == low_group)
                if 1 <= t <= len(tasks):
                    held[t - 1] = weights(*held[t - 1])
                if t >= 2:
                    gather(group_rows(tasks[t - 2][1]), *held.pop(t - 2))
            return carry

        lax.fori_loop(0, tiles // unroll, step, 0)

    def group_rows(g):
        return slice(g * rows_group, (g + 1) * rows_group)

    def send_rows(g):
        for zs in range(g * strips, (g + 1) * strips):
            rows = acc[zs * piece : (zs + 1) * piece]
            mo[zs] = jnp.where(low(half), swap(rows[:half]), rows[half:]).astype(BF16)
        for zs in range(g * strips, (g + 1) * strips):

            @pl.when(z == zs)
            def _():
                m2[zs] = mo[zs]

            @pl.when(z != zs)
            def _():
                d = lax.rem(zs - z + nz, nz) - 1
                remote(mo.at[zs], m2.at[z], m2_s.at[d], m2_r.at[d], sp=zs * 2 + c).start()

    stretch(3, (3,), 4)
    stretch(2, (2, 3), 2)
    serve(3)
    stretch(1, (1, 2, 3), 2)
    serve(4)
    stretch(0, (2, 3), 2)
    send_rows(3)
    send_rows(2)
    serve(5)
    stretch(0, (0, 1), 2)
    send_rows(1)
    send_rows(0)

    own_wo.wait()
    for d in range(1, nx):
        got = wo.at[xat(-d), own_half]
        remote(wo_ref.at[own_half], got, wo_s.at[d - 1], wo_r.at[d - 1], tp=xat(d)).wait_recv()
        copy = remote(got, got, wop_s.at[d - 1], wop_r.at[d - 1], sp=partner)
        copy.start()
        ends.append(copy)
    serve(6)
    other_half = pl.ds(pl.multiple_of((1 - c) * share, share), share)
    for d in range(1, nx):
        there = wo.at[xat(-d), other_half]
        remote(there, there, wop_s.at[d - 1], wop_r.at[d - 1], sp=partner).wait_recv()
    for d in order:
        zs = zat(-d)
        remote(mo.at[z], m2.at[zs], m2_s.at[d - 1], m2_r.at[d - 1], sp=zat(d) * 2 + c).wait_recv()
    serve(7)

    top, bottom = [], []
    keep = low(half)
    for p in range(nz // 2):
        a, b = m2[2 * p].astype(F32), m2[2 * p + 1].astype(F32)
        top.append(jnp.where(keep, a, swap(b)).astype(BF16))
        bottom.append(jnp.where(keep, swap(a), b).astype(BF16))
    mixed = jnp.concatenate(
        [jnp.concatenate(top, axis=1), jnp.concatenate(bottom, axis=1)], axis=0
    )
    loads[6].wait()
    chunk = min(512, width)
    square = jnp.zeros((piece, 1), F32)
    for n in range(width // chunk):
        cols = slice(n * chunk, (n + 1) * chunk)
        weight = wo[:, :, cols].reshape(nx * wo.shape[1], chunk)
        added = resid_ref[:, cols].astype(F32) + jnp.dot(
            mixed, weight, preferred_element_type=F32
        )
        added = added.astype(BF16)
        state[:, cols] = added
        added = added.astype(F32)
        square += jnp.sum(added * added, axis=1, keepdims=True)
    factor = lax.rsqrt(square / width + EPS)
    mine_rows = pl.ds(pl.multiple_of(HALO + x * piece, HALO), piece)
    ext[mine_rows] = (state[...].astype(F32) * factor * gain_ref[...]).astype(BF16)

    sides = (xat(1), xat(-1))
    halves = (slice(0, width // 2), slice(width // 2, width))

    def normed_half(origin, h):
        return ext.at[pl.ds(pl.multiple_of(HALO + origin * piece, HALO), piece), halves[h]]

    def normed_copy(way, h, origin):
        part = normed_half(origin, h)
        return remote(part, part, nx_s.at[way, h], nx_r.at[way, h], tp=sides[way])

    def normed_on(way, origin):
        part = normed_half(origin, way)
        return remote(part, part, nx_s.at[way, 2], nx_r.at[way, 2], tp=sides[way])

    for turn_h in range(2):
        for way in range(2):
            begin(normed_copy(way, turn_h if way == 0 else 1 - turn_h, x))

    rim = ext.at[nx * piece : nx * piece + HALO]
    rims = [
        remote(rim, ext.at[0:HALO], ha_s.at[xp], ha_r, sp=after, tp=xp) for xp in range(nx)
    ]

    @pl.when(last_x)
    def _():
        for copy in rims:
            copy.start()

    serve(8)
    for way in range(2):
        normed_copy(way, way, sides[1 - way]).wait_recv()
        begin(normed_on(way, sides[1 - way]))
    serve(9)
    for way in range(2):
        normed_copy(way, 1 - way, sides[1 - way]).wait_recv()
    for way in range(2):
        normed_on(way, xat(2)).wait_recv()
    rims[0].wait_recv()

    @pl.when(sp == 0)
    def _():
        ext[0:HALO] = jnp.zeros((HALO, width), BF16)

    def all_across(kind):
        for index in range(nz):
            across(zat(-index), kind, index, 1 - c).wait_recv()

    all_across(0)
    all_across(2)

    chunk = min(256, ff)

    def conv(pre, taps, cols):
        pre = pre.astype(BF16).astype(F32)
        count = taps.shape[0]
        total = taps[0:1, cols] * pre[HALO - count + 1 : HALO - count + 1 + tok]
        for i in range(1, count):
            at = HALO - count + 1 + i
            total = total + taps[i : i + 1, cols] * pre[at : at + tok]
        return total

    for n in range(ff // chunk):
        cols = slice(n * chunk, (n + 1) * chunk)
        gate = jnp.dot(ext[...], wf[:, cols], preferred_element_type=F32)
        value = jnp.dot(
            ext[...], wf[:, ff + n * chunk : ff + (n + 1) * chunk], preferred_element_type=F32
        )
        gate = conv(gate, cg_ref, cols)
        value = conv(value, cv_ref, cols)
        gated[:, cols] = (gate / (1.0 + jnp.exp(-gate)) * value).astype(BF16)

    def block_rows(at):
        return pl.ds(pl.multiple_of(at * piece, piece), piece)

    def sum_copy(way, stage, cols):
        at = xat(2) if stage == 0 else sides[way]
        slot = 2 if stage == 0 else way
        return remote(
            rsb.at[block_rows(at), cols], rsr.at[slot, :, cols], rs_s.at[way, stage],
            rs_r.at[way, stage], tp=sides[way],
        )

    all_across(1)
    quarter = nz // 4
    for n in [h * quarter + i for i in range(quarter) for h in range(2)]:
        pair = []
        for zz in (2 * n, 2 * n + 1):
            pair.append(
                jnp.concatenate(
                    [
                        wf[
                            (zz * 2 + cc) * slab : (zz * 2 + cc + 1) * slab,
                            2 * ff + j * LANES : 2 * ff + (j + 1) * LANES,
                        ]
                        for cc in range(2)
                        for j in range(blocks)
                    ],
                    axis=0,
                )
            )
        part = jnp.dot(
            gated[...], jnp.concatenate(pair, axis=1), preferred_element_type=F32
        )
        cols = slice(n * 2 * LANES, (n + 1) * 2 * LANES)
        pf[:, cols] = part
        rsb[:, cols] = part.astype(BF16)
        sum_copy(n // quarter, 0, cols).start()
    for way in range(2):
        begin(sum_copy(way, 1, halves[1 - way]))
    for way in range(2):
        cols = halves[way]
        sum_copy(way, 0, cols).wait_recv()
        rsb[block_rows(sides[way]), cols] = (
            pf[block_rows(sides[way]), cols] + rsr[2, :, cols].astype(F32)
        ).astype(BF16)
        begin(sum_copy(way, 2, cols))
    for h in range(2):
        cols = halves[h]
        sum_copy(1 - h, 1, cols).wait_recv()
        sum_copy(h, 2, cols).wait_recv()
        total = state[:, cols].astype(F32) + pf[block_rows(x), cols]
        total = total + rsr[0, :, cols].astype(F32) + rsr[1, :, cols].astype(F32)
        out_ref[:, cols] = total.astype(BF16)

    for copy in ends:
        copy.wait_send()
    for way in range(2):
        sum_copy(way, 0, halves[way]).wait_send()
    for d in range(1, nz):
        remote(mo.at[zat(d)], m2.at[z], m2_s.at[d - 1], m2_r.at[d - 1], sp=zat(d) * 2 + c).wait_send()
    for e in range(1, nx):
        remote(
            s2.at[:, 0:piece], kv.at[:, c, x], s3_s.at[e - 1], s3_r.at[e - 1], tp=xat(e)
        ).wait_send()
        remote(
            wo_ref.at[own_half], wo.at[x, own_half], wo_s.at[e - 1], wo_r.at[e - 1], tp=xat(e)
        ).wait_send()

    @pl.when(last_x)
    def _():
        for copy in rims:
            copy.wait_send()


def body(*args):
    queries, keys, values, resid, out_weight, gate_weight = args[:6]
    nx, nz = lax.axis_size("tp"), lax.axis_size("sp") // 2
    tok, mix = queries.shape
    piece, width = resid.shape
    ff = gate_weight.shape[1]
    slab = gate_weight.shape[0]
    heads = mix // HEAD
    assert heads * nx == nz and nx == 4
    blocks = ff // 2 // slab
    dims = (nx, nz, heads, tok, piece, width, ff, slab)
    packed = piece + piece // 2
    vmem = pltpu.VMEM
    dma = pltpu.SemaphoreType.DMA
    scratch = [
        vmem((tok, mix), BF16),
        vmem((tok, mix), BF16),
        vmem((tok, mix), BF16),
        vmem((piece, width), BF16),
        vmem((HEAD, ff // 2), BF16),
        vmem((nz * piece, LANES), jnp.int32),
        vmem((nx, heads, packed, LANES), BF16),
        vmem((nx, heads, packed, LANES), BF16),
        vmem((nz, packed, LANES), BF16),
        vmem((nz, 2, nx, piece, LANES), BF16),
        vmem((nz * piece, LANES), BF16),
        vmem((tok, tok), BF16),
        vmem((nz * piece, LANES), F32),
        vmem((nz * piece, LANES), F32),
        vmem((nz, piece // 2, LANES), BF16),
        vmem((nz, piece // 2, LANES), BF16),
        vmem((nx, out_weight.shape[0], width), BF16),
        vmem((2 * nz * slab, 2 * ff + blocks * LANES), BF16),
        vmem((HEAD, ff // 2), BF16),
        vmem((piece, width), BF16),
        vmem((HALO + tok, width), BF16),
        vmem((tok, ff), BF16),
        vmem((tok, width), BF16),
        vmem((tok, width), F32),
        vmem((nx - 1, piece, width), BF16),
    ]
    sems = [
        dma((2, nx - 1)), dma((2, nx - 1)),
        dma((2, nz - 1)), dma((2, nz - 1)),
        dma((nx - 1,)), dma((nx - 1,)),
        dma((nx,)), dma((nx,)),
        dma((7,)),
        dma((2, nz // 2)), dma((2, nz // 2)),
        dma((2, nz // 2)), dma((2, nz // 2)),
        dma((3, nz)), dma((3, nz)),
        dma((nz,)), dma((nz,)),
        dma, dma((nx - 1,)), dma((nx - 1,)),
        dma((nx - 1,)), dma((nx - 1,)),
        dma((nz - 1,)), dma((nz - 1,)),
        dma((2, 3)), dma((2, 3)),
        dma((nx,)), dma,
        dma((2, 3)), dma((2, 3)),
        dma, dma,
    ]
    in_vmem = pl.BlockSpec(memory_space=pltpu.VMEM)
    anywhere = pl.BlockSpec(memory_space=pl.ANY)
    specs = [anywhere] * 7 + [in_vmem] * 3 + [anywhere]
    args = list(args)
    args[9] = args[9].reshape(1, width)
    args[10] = args[10].T
    return pl.pallas_call(
        functools.partial(kernel, dims),
        out_shape=jax.ShapeDtypeStruct((piece, width), BF16),
        in_specs=specs,
        out_specs=in_vmem,
        scratch_shapes=scratch + sems,
        compiler_params=pltpu.CompilerParams(
            collective_id=0, has_side_effects=True, vmem_limit_bytes=66 * 1000 * 1000
        ),
        name="layer",
    )(*args)


def solution(mesh):
    placed = (
        P(("grp", "sp"), "tp"),
        P(("grp", "sp"), "tp"),
        P(("grp", "sp"), "tp"),
        P(("grp", "sp", "tp"), None),
        P("tp", None),
        P("sp", "tp"),
        P("sp", "tp"),
        P(None, "tp"),
        P(None, "tp"),
        P(),
        P("tp", "sp"),
    )
    return jax.shard_map(
        body, mesh=mesh, in_specs=placed, out_specs=P(("grp", "sp", "tp"), None), check_vma=False
    )
```
